32 devices in a mesh: grp: 2 (over y), sp: 4 (over z), tp: 4 (over x, core).
Axes of the slice: x: 2, y: 2, z: 4, core: 2. Of those that a mesh axis runs over, the one named last changes fastest.
Arguments:
- tokens: bfloat16 [1024, 2048], P(('grp', 'sp'), 'tp'), parts along dimension 0, may hold values from -30 to 30, as said below
- norm_gain: float32 [2, 2048], replicated, may hold values from 0.1 to 1.9
- in_weight: bfloat16 [2, 2048, 2048], P(None, 'sp', 'tp'), may hold values from -0.125 to 0.125
- gate_weight: bfloat16 [2, 2048, 2048], P(None, 'sp', 'tp'), may hold values from -0.125 to 0.125
- conv_taps: float32 [2, 4, 2048], P(None, None, 'tp'), may hold values from -3 to 3
- decay_logit: float32 [2, 2, 2048], P(None, None, 'tp'), may hold values from 4 to 20, as said below
- gate_maps: bfloat16 [2, 2048, 1024], P(None, 'tp', 'sp'), may hold values from -0.375 to 0.375
- out_weight: bfloat16 [2, 2048, 2048], P(None, 'sp', 'tp'), may hold values from -0.375 to 0.375
- final_gain: float32 [2048], P('tp'), may hold values from 0.1 to 1.9
Outputs:
- normed_out: bfloat16 [1024, 2048], P(('grp', 'sp'), 'tp'), parts along dimension 0
The draws below stay inside these ranges and needn't reach their ends.
There are 2 independent parts, one for each index of `grp`. The reference program is written for one: setup_inputs(seed, part) draws one part's arguments, and reference() takes and returns one part's arrays. A program takes and returns all parts, laid end to end along the dimension named above; an argument that names none is the same for every part. Nothing has to cross between parts.
Inputs may be any that keep to these rules, and one draw needn't show every extreme that they name: Activations of order one whose scale changes by blocks of tokens and of channels. `decay_logit`: decay parameters; channels differ in how far their state reaches.
All inputs are finite; a program needn't handle non-finite values.
Results may differ from the reference program's by a relative error of at most 0.02.
Values may be sent and summed in bfloat16 or wider, within the bound.
A program may use at most 128 MiB of HBM per device.

```python
import jax
import jax.numpy as jnp
from jax import lax

D = 2048
HEADS = 8
HEAD_W = 256
TAPS = 4
LAYERS = 2
TOK_DEV = 128
WIDTH_R = 2048
TOKENS = 512


def draw_tokens(key, part):
    first, second, third = jax.random.split(key, 3)
    base = jnp.clip(jax.random.normal(first, (TOKENS, D), jnp.float32), -5.0, 5.0)
    span = TOK_DEV // 2
    row_scale = jnp.exp(jax.random.uniform(second, (TOKENS // span,), jnp.float32, jnp.log(0.4), jnp.log(2.0)))
    col_scale = jnp.exp(jax.random.uniform(third, (8,), jnp.float32, jnp.log(0.35), jnp.log(2.8)))
    rows = jnp.repeat(row_scale, span)
    cols = jnp.repeat(col_scale, D // 8)
    return (base * rows[:, None] * cols[None, :]).astype(jnp.bfloat16)


def draw_decay_logit(key, part):
    first, second, third = jax.random.split(key, 3)
    shape = (LAYERS, 2, WIDTH_R)
    share = 0.5
    quick = jax.random.uniform(first, shape, jnp.float32) < share
    slow_rate = jnp.exp(jax.random.uniform(second, shape, jnp.float32, jnp.log(0.02), jnp.log(0.25))) / TOKENS
    quick_rate = jnp.exp(jax.random.uniform(third, shape, jnp.float32, jnp.log(0.0025), jnp.log(0.0083)))
    rate = jnp.where(quick, quick_rate, slow_rate)
    return -jnp.log(jnp.expm1(rate))


def levels(key, extent, pieces, low, high):
    gain, own = 1.0, jax.random.fold_in(key, 6)
    for axis_at, shards_of in pieces:
        heights = jnp.exp(jax.random.uniform(jax.random.fold_in(own, axis_at), (shards_of,), jnp.float32, low / len(pieces), high / len(pieces)))
        gain = gain * jnp.repeat(heights, extent[axis_at] // shards_of).reshape([-1 if axis == axis_at else 1 for axis in range(len(extent))])
    return gain


def bell_draw(rng, shape, spread, most, shards=(), dtype=jnp.bfloat16):
    level = levels(rng, shape, shards, -0.22, 0.18) if shards else 1.0
    values = jax.random.normal(rng, shape, jnp.float32) * spread * level
    return jnp.minimum(jnp.maximum(values, -most), most).astype(dtype)


def setup_inputs(seed: int = 0, part: int = 0) -> dict:
    key_of = jax.random.split(jax.random.key(seed), 10)
    own_keys = jax.random.split(jax.random.fold_in(key_of[9], part), 10)
    return {
        "tokens": draw_tokens(jax.random.fold_in(jax.random.fold_in(key_of[9], part), 71), part),
        "norm_gain": jnp.clip(1.0 + 0.18 * jax.random.normal(key_of[1], (LAYERS, D), jnp.float32), 0.1, 1.9),
        "in_weight": bell_draw(key_of[2], (LAYERS, D, WIDTH_R), D ** -0.5, 0.125, ((1, 4), (2, 4))),
        "gate_weight": bell_draw(key_of[3], (LAYERS, D, WIDTH_R), D ** -0.5, 0.125, ((1, 4), (2, 4))),
        "conv_taps": bell_draw(key_of[4], (LAYERS, TAPS, WIDTH_R), 0.5, 3.0, ((2, 4),), jnp.float32),
        "decay_logit": draw_decay_logit(jax.random.fold_in(key_of[9], 71), part),
        "gate_maps": bell_draw(key_of[6], (LAYERS, WIDTH_R, 4 * HEAD_W), HEAD_W ** -0.5, 0.375, ((1, 4), (2, 4))),
        "out_weight": bell_draw(key_of[7], (LAYERS, WIDTH_R, D), (WIDTH_R // 8) ** -0.5, 0.375, ((1, 4), (2, 4))),
        "final_gain": jnp.clip(1.0 + 0.18 * jax.random.normal(key_of[8], (D,), jnp.float32), 0.1, 1.9),
    }


EPS = 1e-06

def combine_pair(earlier, later):
    return (earlier[0] * later[0], later[0] * earlier[1] + later[1])

def reference(tokens, norm_gain, in_weight, gate_weight, conv_taps, decay_logit, gate_maps, out_weight, final_gain):
    resid = tokens
    length = tokens.shape[0]
    for layer in range(LAYERS):
        wide = resid.astype(jnp.float32)
        normed = (wide * lax.rsqrt(lax.optimization_barrier(jnp.mean(wide * wide, axis=1, keepdims=True)) + EPS) * norm_gain[layer]).astype(jnp.bfloat16)
        xin = jnp.dot(normed, in_weight[layer], preferred_element_type=jnp.float32).astype(jnp.bfloat16)
        gin = jnp.dot(normed, gate_weight[layer], preferred_element_type=jnp.float32).astype(jnp.bfloat16)
        padded = jnp.pad(xin.astype(jnp.float32), ((2, 1), (0, 0)))
        conv = conv_taps[layer, 0] * padded[0:length]
        for k in range(1, TAPS):
            conv = conv + conv_taps[layer, k] * padded[k:k + length]
        conv = conv.astype(jnp.bfloat16)
        stacked = conv.astype(jnp.float32).reshape(length, HEADS, HEAD_W)
        maps = gate_maps[layer].astype(jnp.float32).reshape(HEADS, HEAD_W, 4 * HEAD_W)
        pre = jnp.einsum('thi,hij->thj', stacked, maps).reshape(length, HEADS, 4, HEAD_W)
        conv32 = conv.astype(jnp.float32)
        states = []
        for direction in range(2):
            rate = jax.nn.sigmoid(pre[:, :, 2 * direction]).reshape(length, WIDTH_R)
            inp = jax.nn.sigmoid(pre[:, :, 2 * direction + 1]).reshape(length, WIDTH_R)
            log_a = -8.0 * rate * jax.nn.softplus(-decay_logit[layer, direction])
            decay = jnp.exp(log_a)
            drive = jnp.sqrt(-jnp.expm1(2.0 * log_a)) * inp * conv32
            _, state = lax.associative_scan(combine_pair, (decay, drive), reverse=direction == 1, axis=0)
            states.append(state)
        mix = (jax.nn.gelu(gin.astype(jnp.float32)) * (states[0] + states[1])).astype(jnp.bfloat16)
        out = jnp.dot(mix, out_weight[layer], preferred_element_type=jnp.float32)
        resid = (resid.astype(jnp.float32) + out).astype(jnp.bfloat16)
    wide = resid.astype(jnp.float32)
    return (wide * lax.rsqrt(lax.optimization_barrier(jnp.mean(wide * wide, axis=1, keepdims=True)) + EPS) * final_gain).astype(jnp.bfloat16)
```

```python
import jax
import jax.numpy as jnp
from jax import lax
from jax.experimental import pallas as pl
from jax.experimental.pallas import tpu as pltpu
from jax.sharding import PartitionSpec as P

D = 2048
HEAD_W = 256
TAPS = 4
LAYERS = 2


EPS = 1e-06


def extended(value, sides, width):
    for axis, dim in sides:
        devices, length = (lax.axis_size(axis), value.shape[dim])
        up = [(i, (i + 1) % devices) for i in range(devices - 1)]
        down = [(j, i) for i, j in up]
        last = lax.slice_in_dim(value, length - width, length, axis=dim)
        leading = lax.slice_in_dim(value, 0, width, axis=dim)
        before = lax.ppermute(last, axis, up)
        after = lax.ppermute(leading, axis, down)
        value = jnp.concatenate([before, value, after], axis=dim)
    return value


def combine_pair(earlier, later):
    return (earlier[0] * later[0], later[0] * earlier[1] + later[1])


def body(
    tokens,
    norm_gain,
    in_weight,
    gate_weight,
    conv_taps,
    decay_logit,
    gate_maps,
    out_weight,
    final_gain,
):
    resid = tokens
    rows = tokens.shape[0]
    width = in_weight.shape[2]
    local_heads = width // HEAD_W
    for layer in range(LAYERS):
        whole = lax.all_gather(resid, "tp", axis=1, tiled=True)
        wide = whole.astype(jnp.float32)
        normed = (
            wide * lax.rsqrt(jnp.mean(wide * wide, axis=1, keepdims=True) + EPS) * norm_gain[layer]
        ).astype(jnp.bfloat16)
        proj_in = jnp.dot(
            normed,
            lax.all_gather(in_weight[layer], "sp", axis=0, tiled=True),
            preferred_element_type=jnp.float32,
        )
        proj_gate = jnp.dot(
            normed,
            lax.all_gather(gate_weight[layer], "sp", axis=0, tiled=True),
            preferred_element_type=jnp.float32,
        )
        xin = proj_in.astype(jnp.bfloat16)
        gin = proj_gate.astype(jnp.bfloat16)
        padded = extended(xin, (("sp", 0),), 2).astype(jnp.float32)
        conv = conv_taps[layer, 0] * padded[0:rows]
        for k in range(1, TAPS):
            conv = conv + conv_taps[layer, k] * padded[k : k + rows]
        conv = conv.astype(jnp.bfloat16)
        stacked = conv.reshape(rows, local_heads, HEAD_W)
        piece = lax.all_gather(gate_maps[layer], "sp", axis=1, tiled=True)
        blocks = piece.reshape(local_heads, HEAD_W, piece.shape[1])
        pre = jnp.einsum("thi,hij->thj", stacked, blocks, preferred_element_type=jnp.float32)
        pre = pre.reshape(rows, local_heads, 4, HEAD_W)
        conv32 = conv.astype(jnp.float32)
        locals_a = []
        locals_h = []
        for direction in range(2):
            rate = jax.nn.sigmoid(pre[:, :, 2 * direction]).reshape(rows, width)
            inp = jax.nn.sigmoid(pre[:, :, 2 * direction + 1]).reshape(rows, width)
            log_a = -8.0 * rate * jax.nn.softplus(-decay_logit[layer, direction])
            decay = jnp.exp(log_a)
            drive = jnp.sqrt(-jnp.expm1(2.0 * log_a)) * inp * conv32
            prod_a, state = lax.associative_scan(
                combine_pair, (decay, drive), reverse=direction == 1, axis=0
            )
            locals_a.append(prod_a)
            locals_h.append(state)
        summary = jnp.stack([locals_a[0][-1], locals_h[0][-1], locals_a[1][0], locals_h[1][0]])[
            None
        ]
        every = lax.all_gather(summary, "sp", axis=0, tiled=True)
        count = every.shape[0]
        me = lax.axis_index("sp")
        _, incl_f = lax.associative_scan(combine_pair, (every[:, 0], every[:, 1]), axis=0)
        _, incl_b = lax.associative_scan(
            combine_pair, (every[:, 2], every[:, 3]), reverse=True, axis=0
        )
        before = lax.dynamic_index_in_dim(incl_f, jnp.maximum(me - 1, 0), 0, keepdims=False)
        after = lax.dynamic_index_in_dim(incl_b, jnp.minimum(me + 1, count - 1), 0, keepdims=False)
        carry_f = before * (me > 0).astype(jnp.float32)
        carry_b = after * (me < count - 1).astype(jnp.float32)
        hidden = locals_h[0] + locals_a[0] * carry_f + locals_h[1] + locals_a[1] * carry_b
        mix = (jax.nn.gelu(gin.astype(jnp.float32)) * hidden).astype(jnp.bfloat16)
        full_mix = lax.all_gather(mix, "tp", axis=1, tiled=True)
        out = jnp.dot(
            full_mix,
            lax.all_gather(out_weight[layer], "sp", axis=0, tiled=True),
            preferred_element_type=jnp.float32,
        )
        resid = (resid.astype(jnp.float32) + out).astype(jnp.bfloat16)
    wide = resid.astype(jnp.float32)
    total = lax.psum(jnp.sum(wide * wide, axis=1), "tp")
    scale = lax.rsqrt(total / D + EPS)
    return (wide * scale[:, None] * final_gain).astype(jnp.bfloat16)


LANES = 128
UNITS = 4
IN, GATE, OUT, MAPS = range(4)
TILE = 256
BF16 = jnp.bfloat16
F32 = jnp.float32


def shifted(value, k, fill, reverse):
    pad = jnp.full((k, value.shape[1]), fill, value.dtype)
    if reverse:
        return jnp.concatenate([value[k:], pad], axis=0)
    return jnp.concatenate([pad, value[:-k]], axis=0)


def scan_rows(decay, state, reverse):
    k, rows = 1, decay.shape[0]
    while k < rows:
        state = state + decay * shifted(state, k, 0.0, reverse)
        if 2 * k < rows:
            decay = decay * shifted(decay, k, 1.0, reverse)
        k *= 2
    return state


def one_minus_exp_neg(u):
    series = u * (1 - u / 2 * (1 - u / 3 * (1 - u / 4 * (1 - u / 5 * (1 - u / 6 * (1 - u / 7))))))
    return jnp.where(u < 0.3, series, 1.0 - jnp.exp(-u))


def kernel(
    S,
    T,
    tok_ref,
    gain_ref,
    in_ref,
    gate_ref,
    taps_ref,
    logit_ref,
    map_ref,
    outw_ref,
    fgain_ref,
    out_ref,
    full,
    normed,
    wbuf,
    mbuf,
    tapb,
    logb,
    proj,
    padded,
    convb,
    fin,
    ssq,
    wss,
    wrs,
    yss,
    yrs,
    zss,
    zrs,
    xss,
    xrs,
    css,
    crs,
    vss,
    vrs,
    pss,
    prs,
    fss,
    frs,
    qss,
    qrs,
    lsem,
):
    g = lax.axis_index("grp")
    s = lax.axis_index("sp")
    t = lax.axis_index("tp")
    c = t % 2
    tc = t + 1 - 2 * c
    tx = (t + 2) % T
    rows, tcols = tok_ref.shape
    tokens = rows * S
    half = in_ref.shape[1] // 2

    def slice_of(ss, tt):
        return 2 * (S * (tt // 2) + ss) + tt % 2

    def lanes(i):
        return pl.ds(pl.multiple_of(i * LANES, LANES), LANES)

    mine = slice_of(s, t)
    home = mine // T
    sub = mine % T

    def owner(q):
        j = T * t + q
        return (j // 2) % S, 2 * (j // (2 * S)) + j % 2

    barrier = pltpu.get_barrier_semaphore()
    for ds in range(S):
        for dt in range(T):
            if ds or dt:
                pl.semaphore_signal(
                    barrier,
                    inc=1,
                    device_id={"sp": (s + ds) % S, "tp": (t + dt) % T},
                    device_id_type=pl.DeviceIdType.MESH,
                )
    pl.semaphore_signal(
        barrier, inc=1, device_id={"grp": 1 - g}, device_id_type=pl.DeviceIdType.MESH
    )
    pl.semaphore_wait(barrier, S * T)

    def remote(src, dst, ssem, rsem, dev):
        return pltpu.make_async_remote_copy(
            src_ref=src,
            dst_ref=dst,
            send_sem=ssem,
            recv_sem=rsem,
            device_id=dev,
            device_id_type=pl.DeviceIdType.MESH,
        )

    def weights_at(layer, kind):
        return mbuf.at[layer] if kind == MAPS else wbuf.at[layer, kind]

    def wcopy(layer, kind, q, part, source, dev):
        if kind == MAPS:
            src = map_ref.at[
                layer, pl.ds((q // 2) * HEAD_W + part * LANES, LANES), pl.ds((q % 2) * LANES, LANES)
            ]
        else:
            src = (in_ref, gate_ref, outw_ref)[kind].at[
                layer, pl.ds(part * half, half), pl.ds(q * LANES, LANES)
            ]
        dst = weights_at(layer, kind).at[source, part]
        rsem = wrs.at[layer, kind, source]
        if dev is None:
            return pltpu.make_async_copy(src, dst, rsem)
        return remote(src, dst, wss.at[layer, kind], rsem, {"sp": dev[0], "tp": dev[1]})

    def weights_start(layer, kind):
        for q in range(T):
            ds, dt = owner(q)

            @pl.when(ds != s)
            def _():
                wcopy(layer, kind, q, g, s, owner(q)).start()

            @pl.when(jnp.logical_and(ds == s, dt == t))
            def _():
                for part in range(2):
                    wcopy(layer, kind, q, part, s, None).start()

            @pl.when(jnp.logical_and(ds == s, dt != t))
            def _():
                for part in range(2):
                    wcopy(layer, kind, q, part, s, owner(q)).start()

    def bulk(ref, sem):
        pltpu.make_async_copy(ref, ref, sem).wait()

    def forward(layer, kind, source):
        at = weights_at(layer, kind).at[source, g]
        return remote(at, at, yss.at[layer, kind], yrs.at[layer, kind], {"grp": 1 - g})

    def weights_forward(layer, kind, d):
        for source in (s - d, s + d):

            @pl.when(jnp.logical_and(source >= 0, source < S))
            def _():
                bulk(weights_at(layer, kind).at[source, g], wrs.at[layer, kind, source])
                forward(layer, kind, source).start()

    def weights_forward_all(layer, kind):
        @pl.loop(1, S)
        def _(d):
            weights_forward(layer, kind, d)

    def weights_wait(layer, kind):
        buf = weights_at(layer, kind)
        bulk(buf.at[s], wrs.at[layer, kind, s])
        bulk(buf.at[pl.ds(0, S - 1), 1 - g], yrs.at[layer, kind])

    def weights_drain(layer, kind):
        buf = weights_at(layer, kind)
        bulk(buf.at[pl.ds(0, T // 2)], wss.at[layer, kind])
        bulk(buf.at[pl.ds(0, S - 1), g], yss.at[layer, kind])

    part_units = 0
    late_units = UNITS - part_units
    units = UNITS + part_units

    def region(gi, ss, tt, u):
        row = jnp.where(gi == 0, ss, u) * rows
        col = jnp.where(gi == 0, tt * UNITS + u, slice_of(ss, tt))
        return full.at[gi, pl.ds(pl.multiple_of(row, rows), rows), lanes(col)]

    def zcopy(gi, b, m, up):
        far = m // UNITS
        at = region(gi, b, (t + 2 * far) % T, m - far * part_units)
        dev = (s + 1) % S if up else (s + S - 1) % S
        return remote(at, at, zss.at[gi, up], zrs.at[gi, b, m], {"sp": dev})

    def xcopy(gi, b, u, tt):
        at = region(gi, b, tt, u)
        return remote(at, at, xss.at[gi], xrs.at[gi, b, u], {"tp": tx})

    def ccopy(gi, b, u, tt):
        at = region(gi, b, tt, u)
        return remote(at, at, css.at[gi], crs.at[gi], {"tp": tc})

    def both_ways(gi, m):
        @pl.when(s + 1 < S)
        def _():
            zcopy(gi, s, m, 1).start()

        @pl.when(s > 0)
        def _():
            zcopy(gi, s, m, 0).start()

    def gather(gi, hook, tail):
        for u in range(late_units, UNITS):
            xcopy(gi, s, u, t).start()

        @pl.loop(0, UNITS)
        def _(m):
            both_ways(gi, m)

        for u in range(late_units):
            xcopy(gi, s, u, t).start()

        @pl.loop(0, UNITS)
        def _(u):
            ccopy(gi, s, u, t).start()

        hook(0)

        for i in range(part_units):
            xcopy(gi, s, late_units + i, tx).wait_recv()
            both_ways(gi, UNITS + i)
            ccopy(gi, s, late_units + i, tx).start()

        def hop(b, up, m):
            far = m // UNITS
            u = m - far * part_units
            zcopy(gi, b, m, up).wait_recv()

            @pl.when((s + 1 < S) if up else (s > 0))
            def _():
                zcopy(gi, b, m, up).start()

            @pl.when(m < late_units)
            def _():
                xcopy(gi, b, u, t).start()

            ccopy(gi, b, u, (t + 2 * far) % T).start()

        def across(b):
            @pl.when(jnp.logical_and(b >= 0, b < S))
            def _():
                for u in range(late_units):
                    xcopy(gi, b, u, tx).wait_recv()
                    ccopy(gi, b, u, tx).start()

        @pl.loop(1, S)
        def _(d):
            @pl.loop(0, units)
            def _(m):
                @pl.when(s - d >= 0)
                def _():
                    hop(s - d, 1, m)

                @pl.when(s + d < S)
                def _():
                    hop(s + d, 0, m)

            across(s - d + 1)

            @pl.when(d > 1)
            def _():
                across(s + d - 1)

            hook(d)

        tail()
        across(s - S + 1)
        across(s + S - 1)
        bulk(full.at[gi, :, pl.ds(0, D // 2)], crs.at[gi])

    def gather_drain(gi):
        for k in range(S - 1):

            @pl.when(s == k)
            def _():
                bulk(full.at[gi, pl.ds(0, rows), pl.ds(0, (k + 1) * units * LANES)], zss.at[gi, 1])

            @pl.when(s == S - 1 - k)
            def _():
                bulk(full.at[gi, pl.ds(0, rows), pl.ds(0, (k + 1) * units * LANES)], zss.at[gi, 0])

        bulk(full.at[gi, pl.ds(0, rows), pl.ds(0, (UNITS + (S - 1) * late_units) * LANES)], xss.at[gi])
        bulk(full.at[gi, :, pl.ds(0, D // 2)], css.at[gi])

    place = full.at[
        0,
        pl.ds(pl.multiple_of(s * rows, rows), rows),
        pl.ds(pl.multiple_of(t * tcols, tcols), tcols),
    ]
    own = pltpu.make_async_copy(tok_ref, place, lsem.at[0])
    own.start()
    tapb[c] = taps_ref[...]
    logb[c] = logit_ref[...]
    pcopies = [
        remote(ref, buf.at[c], pss.at[i], prs.at[i], {"tp": tc})
        for i, (ref, buf) in enumerate(((taps_ref, tapb), (logit_ref, logb)))
    ]
    for copy in pcopies:
        copy.start()
    own.wait()
    depth = S * 2 * half
    step = 64

    def first_half(layer, gi):
        @pl.loop(0, tokens // step)
        def _(i):
            at = pl.ds(pl.multiple_of(i * step, step), step)
            wide = full[gi, at, :].astype(F32)
            scale = lax.rsqrt(jnp.mean(wide * wide, axis=1, keepdims=True) + EPS)
            normed[at, :] = (wide * scale * gain_ref[pl.ds(layer, 1), :]).astype(BF16)

        weights_wait(layer, IN)

        @pl.loop(0, tokens // TILE)
        def _(i):
            at = pl.ds(pl.multiple_of(i * TILE, TILE), TILE)
            xin = jnp.dot(
                normed[at, :], wbuf[layer, IN].reshape(depth, LANES), preferred_element_type=F32
            )
            padded[pl.ds(pl.multiple_of(i * TILE + 8, 8), TILE), :] = xin.astype(BF16).astype(F32)

        @pl.when(layer == 0)
        def _():
            for copy in pcopies:
                copy.wait()

        par = tapb[home % 2, layer, :, lanes(sub)]
        rates = jax.nn.softplus(-logb[home % 2, layer, :, lanes(sub)])
        edge = jnp.zeros((8, LANES), F32)
        padded[0:8, :] = edge
        padded[tokens + 8 : tokens + 16, :] = edge
        conv = par[0:1] * padded[6 : 6 + tokens, :]
        for k in range(1, TAPS):
            conv = conv + par[k : k + 1] * padded[6 + k : 6 + k + tokens, :]
        convb[layer, c] = conv.astype(BF16)
        vcopy = remote(
            convb.at[layer, c], convb.at[layer, c], vss.at[layer], vrs.at[layer], {"tp": tc}
        )
        vcopy.start()
        weights_forward_all(layer, MAPS)
        weights_forward_all(layer, OUT)
        weights_wait(layer, MAPS)
        vcopy.wait()
        both = jnp.concatenate([convb[layer, 0], convb[layer, 1]], axis=1)
        conv32 = convb[layer, c].astype(F32)
        hidden = None
        for d in range(2):
            pair = []
            for k in (2 * d, 2 * d + 1):
                weight = mbuf[layer, k].reshape(HEAD_W, LANES)
                pair.append(jax.nn.sigmoid(jnp.dot(both, weight, preferred_element_type=F32)))
            log_a = -8.0 * pair[0] * rates[d : d + 1]
            drive = jnp.sqrt(one_minus_exp_neg(-2.0 * log_a)) * pair[1] * conv32
            state = scan_rows(jnp.exp(log_a), drive, d == 1)
            hidden = state if hidden is None else hidden + state
            pass
        proj[...] = hidden
        weights_wait(layer, GATE)

        @pl.loop(0, tokens // TILE)
        def _(i):
            at = pl.ds(pl.multiple_of(i * TILE, TILE), TILE)
            gin = jnp.dot(
                normed[at, :], wbuf[layer, GATE].reshape(depth, LANES), preferred_element_type=F32
            )
            gin = gin.astype(BF16).astype(F32)
            full[gi + 1, at, lanes(mine)] = (jax.nn.gelu(gin) * proj[at, :]).astype(BF16)

    def second_half(layer, gi):
        weights_wait(layer, OUT)

        @pl.loop(0, tokens // TILE)
        def _(i):
            at = pl.ds(pl.multiple_of(i * TILE, TILE), TILE)
            prod = jnp.dot(
                full[gi, at, :], wbuf[layer, OUT].reshape(depth, LANES), preferred_element_type=F32
            )
            old = full[gi - 1, at, lanes(mine)]
            full[gi + 1, at, lanes(mine)] = (old.astype(F32) + prod).astype(BF16)

    @pl.loop(0, 2 * LAYERS)
    def _(gi):
        layer = gi // 2
        more = layer + 1 < LAYERS

        def hook(d):
            @pl.when(gi % 2 == 0)
            def _():
                if isinstance(d, int):
                    @pl.when(gi == 0)
                    def _():
                        weights_start(layer, IN)
                    @pl.when(gi == 0)
                    def _():
                        weights_start(layer, GATE)
                else:
                    @pl.when(jnp.logical_and(gi == 0, d == 2))
                    def _():
                        weights_start(layer, MAPS)
                    weights_forward(layer, IN, d)
                    weights_forward(layer, GATE, d)

            @pl.when(gi % 2 == 1)
            def _():
                pass

        def tail():
            @pl.when(gi % 2 == 0)
            def _():
                weights_start(layer, OUT)
            @pl.when(jnp.logical_and(gi % 2 == 0, more))
            def _():
                weights_start(layer + 1, IN)
                weights_start(layer + 1, GATE)
            @pl.when(jnp.logical_and(gi % 2 == 1, more))
            def _():
                weights_start(layer + 1, MAPS)

        gather(gi, hook, tail)

        @pl.when(gi % 2 == 0)
        def _():
            first_half(gi // 2, gi)

        @pl.when(gi % 2 == 1)
        def _():
            second_half(gi // 2, gi)

    def fcopy(ss, q, dev):
        src = full.at[2 * LAYERS, pl.ds(pl.multiple_of(ss * rows, rows), rows), lanes(mine)]
        dst = fin.at[:, lanes(q)]
        if dev is None:
            return pltpu.make_async_copy(src, dst, frs.at[q])
        return remote(src, dst, fss.at[ss], frs.at[q], dev)

    for d in range(S):
        ss = (s + d) % S
        same = jnp.logical_and(ss == s, home == t)

        @pl.when(same)
        def _():
            fcopy(ss, sub, None).start()

        @pl.when(jnp.logical_not(same))
        def _():
            fcopy(ss, sub, {"sp": ss, "tp": home}).start()

    for q in range(T):
        fcopy(0, q, None).wait()
    wide = fin[...].astype(F32)
    sums = jnp.broadcast_to(jnp.sum(wide * wide, axis=1, keepdims=True), (rows, LANES))
    ssq[t] = sums.T[0:8]

    def qcopy(source, d):
        return remote(
            ssq.at[source], ssq.at[source], qss.at[d], qrs.at[source], {"tp": (t + d) % T}
        )

    for d in range(1, T):
        qcopy(t, d).start()
    for d in range(1, T):
        qcopy((t + d) % T, d).wait_recv()
    total = ssq[0]
    for i in range(1, T):
        total = total + ssq[i]
    total = jnp.broadcast_to(total[0:1], (LANES, rows)).T[:, 0:1]
    out_ref[...] = (fin[...].astype(F32) * lax.rsqrt(total / D + EPS) * fgain_ref[...]).astype(BF16)

    for gi in range(2 * LAYERS):
        gather_drain(gi)
    for layer in range(LAYERS):
        for kind in range(4):
            weights_drain(layer, kind)
    for ss in range(S):

        @pl.when(jnp.logical_not(jnp.logical_and(s == ss, home == t)))
        def _():
            fcopy(ss, sub, {"sp": ss, "tp": home}).wait_send()

    for d in range(1, T):
        qcopy(t, d).wait_send()


def fused(mesh):
    S, T = mesh.shape["sp"], mesh.shape["tp"]

    def run(tokens, norm_gain, in_weight, gate_weight, conv_taps, decay_logit, gate_maps, out_weight, final_gain):
        rows, tcols = tokens.shape
        total = rows * S
        half = in_weight.shape[1] // 2
        dma = pltpu.SemaphoreType.DMA
        n = 2 * LAYERS
        vmem = pl.BlockSpec(memory_space=pltpu.VMEM)
        hbm = pl.BlockSpec(memory_space=pl.ANY)

        def body_of(*refs):
            kernel(S, T, *refs)

        return pl.pallas_call(
            body_of,
            out_shape=jax.ShapeDtypeStruct((rows, tcols), BF16),
            in_specs=[hbm, vmem, hbm, hbm, vmem, vmem, hbm, hbm, vmem],
            out_specs=vmem,
            scratch_shapes=[
                pltpu.VMEM((n + 1, total, D), BF16),
                pltpu.VMEM((total, D), BF16),
                pltpu.VMEM((LAYERS, 3, S, 2, half, LANES), BF16),
                pltpu.VMEM((LAYERS, S, 2, LANES, LANES), BF16),
                pltpu.VMEM((2, LAYERS, TAPS, tcols), F32),
                pltpu.VMEM((2, LAYERS, 2, tcols), F32),
                pltpu.VMEM((total, LANES), F32),
                pltpu.VMEM((total + 16, LANES), F32),
                pltpu.VMEM((LAYERS, 2, total, LANES), BF16),
                pltpu.VMEM((rows, tcols), BF16),
                pltpu.VMEM((T, 8, rows), F32),
                dma((LAYERS, 4)),
                dma((LAYERS, 4, S)),
                dma((LAYERS, 4)),
                dma((LAYERS, 4)),
                dma((n, 2)),
                dma((n, S, UNITS + 1)),
                dma((n,)),
                dma((n, S, UNITS)),
                dma((n,)),
                dma((n,)),
                dma((LAYERS,)),
                dma((LAYERS,)),
                dma((2,)),
                dma((2,)),
                dma((S,)),
                dma((T,)),
                dma((T,)),
                dma((T,)),
                dma((1,)),
            ],
            compiler_params=pltpu.CompilerParams(
                collective_id=0, has_side_effects=True, vmem_limit_bytes=60 * 1024 * 1024
            ),
        )(tokens, norm_gain, in_weight, gate_weight, conv_taps, decay_logit, gate_maps, out_weight, final_gain.reshape(1, tcols))

    return run


def solution(mesh):
    placed = (
        P(("grp", "sp"), "tp"),
        P(),
        P(None, "sp", "tp"),
        P(None, "sp", "tp"),
        P(None, None, "tp"),
        P(None, None, "tp"),
        P(None, "tp", "sp"),
        P(None, "sp", "tp"),
        P("tp"),
    )
    shape = dict(mesh.shape)
    fits = (
        shape["grp"] == 2
        and shape["tp"] == 4
        and shape["sp"] == 4
        and D == shape["sp"] * shape["tp"] * LANES
        and HEAD_W == 2 * LANES
    )
    return jax.shard_map(
        fused(mesh) if fits else body, mesh=mesh, in_specs=placed, out_specs=P(("grp", "sp"), "tp"), check_vma=False
    )
```

```python
import jax
import jax.numpy as jnp
from jax import lax
from jax.experimental import pallas as pl
from jax.experimental.pallas import tpu as pltpu
from jax.sharding import PartitionSpec as P

D = 2048
HEAD_W = 256
TAPS = 4
LAYERS = 2


EPS = 1e-06


def extended(value, sides, width):
    for axis, dim in sides:
        devices, length = (lax.axis_size(axis), value.shape[dim])
        up = [(i, (i + 1) % devices) for i in range(devices - 1)]
        down = [(j, i) for i, j in up]
        last = lax.slice_in_dim(value, length - width, length, axis=dim)
        leading = lax.slice_in_dim(value, 0, width, axis=dim)
        before = lax.ppermute(last, axis, up)
        after = lax.ppermute(leading, axis, down)
        value = jnp.concatenate([before, value, after], axis=dim)
    return value


def combine_pair(earlier, later):
    return (earlier[0] * later[0], later[0] * earlier[1] + later[1])


def body(
    tokens,
    norm_gain,
    in_weight,
    gate_weight,
    conv_taps,
    decay_logit,
    gate_maps,
    out_weight,
    final_gain,
):
    resid = tokens
    rows = tokens.shape[0]
    width = in_weight.shape[2]
    local_heads = width // HEAD_W
    for layer in range(LAYERS):
        whole = lax.all_gather(resid, "tp", axis=1, tiled=True)
        wide = whole.astype(jnp.float32)
        normed = (
            wide * lax.rsqrt(jnp.mean(wide * wide, axis=1, keepdims=True) + EPS) * norm_gain[layer]
        ).astype(jnp.bfloat16)
        proj_in = jnp.dot(
            normed,
            lax.all_gather(in_weight[layer], "sp", axis=0, tiled=True),
            preferred_element_type=jnp.float32,
        )
        proj_gate = jnp.dot(
            normed,
            lax.all_gather(gate_weight[layer], "sp", axis=0, tiled=True),
            preferred_element_type=jnp.float32,
        )
        xin = proj_in.astype(jnp.bfloat16)
        gin = proj_gate.astype(jnp.bfloat16)
        padded = extended(xin, (("sp", 0),), 2).astype(jnp.float32)
        conv = conv_taps[layer, 0] * padded[0:rows]
        for k in range(1, TAPS):
            conv = conv + conv_taps[layer, k] * padded[k : k + rows]
        conv = conv.astype(jnp.bfloat16)
        stacked = conv.reshape(rows, local_heads, HEAD_W)
        piece = lax.all_gather(gate_maps[layer], "sp", axis=1, tiled=True)
        blocks = piece.reshape(local_heads, HEAD_W, piece.shape[1])
        pre = jnp.einsum("thi,hij->thj", stacked, blocks, preferred_element_type=jnp.float32)
        pre = pre.reshape(rows, local_heads, 4, HEAD_W)
        conv32 = conv.astype(jnp.float32)
        locals_a = []
        locals_h = []
        for direction in range(2):
            rate = jax.nn.sigmoid(pre[:, :, 2 * direction]).reshape(rows, width)
            inp = jax.nn.sigmoid(pre[:, :, 2 * direction + 1]).reshape(rows, width)
            log_a = -8.0 * rate * jax.nn.softplus(-decay_logit[layer, direction])
            decay = jnp.exp(log_a)
            drive = jnp.sqrt(-jnp.expm1(2.0 * log_a)) * inp * conv32
            prod_a, state = lax.associative_scan(
                combine_pair, (decay, drive), reverse=direction == 1, axis=0
            )
            locals_a.append(prod_a)
            locals_h.append(state)
        summary = jnp.stack([locals_a[0][-1], locals_h[0][-1], locals_a[1][0], locals_h[1][0]])[
            None
        ]
        every = lax.all_gather(summary, "sp", axis=0, tiled=True)
        count = every.shape[0]
        me = lax.axis_index("sp")
        _, incl_f = lax.associative_scan(combine_pair, (every[:, 0], every[:, 1]), axis=0)
        _, incl_b = lax.associative_scan(
            combine_pair, (every[:, 2], every[:, 3]), reverse=True, axis=0
        )
        before = lax.dynamic_index_in_dim(incl_f, jnp.maximum(me - 1, 0), 0, keepdims=False)
        after = lax.dynamic_index_in_dim(incl_b, jnp.minimum(me + 1, count - 1), 0, keepdims=False)
        carry_f = before * (me > 0).astype(jnp.float32)
        carry_b = after * (me < count - 1).astype(jnp.float32)
        hidden = locals_h[0] + locals_a[0] * carry_f + locals_h[1] + locals_a[1] * carry_b
        mix = (jax.nn.gelu(gin.astype(jnp.float32)) * hidden).astype(jnp.bfloat16)
        full_mix = lax.all_gather(mix, "tp", axis=1, tiled=True)
        out = jnp.dot(
            full_mix,
            lax.all_gather(out_weight[layer], "sp", axis=0, tiled=True),
            preferred_element_type=jnp.float32,
        )
        resid = (resid.astype(jnp.float32) + out).astype(jnp.bfloat16)
    wide = resid.astype(jnp.float32)
    total = lax.psum(jnp.sum(wide * wide, axis=1), "tp")
    scale = lax.rsqrt(total / D + EPS)
    return (wide * scale[:, None] * final_gain).astype(jnp.bfloat16)


LANES = 128
IN, GATE, OUT, MAPS = range(4)
BF16 = jnp.bfloat16
F32 = jnp.float32


def shifted(value, k, fill, reverse):
    pad = jnp.full((k, value.shape[1]), fill, value.dtype)
    if reverse:
        return jnp.concatenate([value[k:], pad], axis=0)
    return jnp.concatenate([pad, value[:-k]], axis=0)


def scan_rows(decay, state, reverse):
    k, rows = 1, decay.shape[0]
    while k < rows:
        state = state + decay * shifted(state, k, 0.0, reverse)
        if 2 * k < rows:
            decay = decay * shifted(decay, k, 1.0, reverse)
        k *= 2
    return state


def one_minus_exp_neg(u):
    series = u * (1 - u / 2 * (1 - u / 3 * (1 - u / 4 * (1 - u / 5 * (1 - u / 6 * (1 - u / 7))))))
    return jnp.where(u < 0.3, series, 1.0 - jnp.exp(-u))


def kernel(
    S,
    T,
    tok_ref,
    gain_ref,
    in_ref,
    gate_ref,
    taps_ref,
    logit_ref,
    map_ref,
    outw_ref,
    fgain_ref,
    out_ref,
    full,
    tokb,
    xg,
    wbuf,
    mbuf,
    tapb,
    logb,
    ownb,
    part,
    peer,
    ssq,
    scaleb,
    padded,
    convb,
    hid,
    last,
    sfin,
    ssqf,
    fin,
    ws,
    wr,
    ys,
    yr,
    us,
    ur,
    cs,
    cr,
    ps,
    pr,
    rs,
    rr,
    vss,
    vrs,
    pss,
    prs,
    fss,
    frs,
    qss,
    qrs,
    lsem,
):
    g = lax.axis_index("grp")
    s = lax.axis_index("sp")
    t = lax.axis_index("tp")
    x, c = t // 2, t % 2
    hf, zl = s // 2, s % 2
    sz = s + 1 - 2 * zl
    sp = (s + 2) % S
    tx = (t + 2) % T
    tc = t + 1 - 2 * c
    rows, tcols = tok_ref.shape
    tokens = rows * S
    depth = full.shape[2]
    block = 2 * hf + x
    sub = 2 * zl + c
    mine = T * x + sub
    holder = x == hf

    def lanes(i, n=1):
        return pl.ds(pl.multiple_of(i * LANES, LANES), n * LANES)

    def rows_at(b):
        return pl.ds(pl.multiple_of(b * rows, rows), rows)

    def remote(src, dst, ssem, rsem, dev):
        return pltpu.make_async_remote_copy(
            src_ref=src,
            dst_ref=dst,
            send_sem=ssem,
            recv_sem=rsem,
            device_id=dev,
            device_id_type=pl.DeviceIdType.MESH,
        )

    def bulk(ref, sem):
        pltpu.make_async_copy(ref, ref, sem).wait()

    def both(a, b):
        return jnp.logical_and(a, b)

    barrier = pltpu.get_barrier_semaphore()
    for ds in range(S):
        for dt in range(T):
            if ds or dt:
                pl.semaphore_signal(
                    barrier,
                    inc=1,
                    device_id={"sp": (s + ds) % S, "tp": (t + dt) % T},
                    device_id_type=pl.DeviceIdType.MESH,
                )

    pl.semaphore_signal(
        barrier, inc=1, device_id={"grp": 1 - g}, device_id_type=pl.DeviceIdType.MESH
    )

    piece = lanes(T * c, T)
    own_full = pltpu.make_async_copy(tok_ref, full.at[0, rows_at(s), piece], lsem.at[0])
    own_side = pltpu.make_async_copy(tok_ref, tokb, lsem.at[0])

    @pl.when(holder)
    def _():
        own_full.start()

    @pl.when(jnp.logical_not(holder))
    def _():
        own_side.start()

    pl.semaphore_wait(barrier, S * T)

    def param_copies(k):
        dev = {"tp": 2 * c + k}
        return [
            remote(ref, buf, pss.at[i, k], prs.at[i], dev)
            for i, (ref, buf) in enumerate(((taps_ref, tapb), (logit_ref, logb)))
        ]

    for k in range(2):

        @pl.when(both(holder, 2 * c + k != t))
        def _():
            for copy in param_copies(k):
                copy.start()

    @pl.when(block == t)
    def _():
        tapb[...] = taps_ref[...]
        logb[...] = logit_ref[...]

    def params_wait():
        @pl.when(block != t)
        def _():
            for copy in param_copies(0):
                copy.wait_recv()

    half = in_ref.shape[1] // 2

    def segment(layer, kind, i, part):
        if kind == MAPS:
            return mbuf.at[layer, i, part]
        return wbuf.at[layer, kind, i // 2, part, :, lanes(i % 2)]

    def wcopy(layer, kind, q, part, local):
        if kind == MAPS:
            src = map_ref.at[
                layer, pl.ds((q // 2) * HEAD_W + part * LANES, LANES), pl.ds((q % 2) * LANES, LANES)
            ]
            i, plane = s, 2 * x + q // 2
        else:
            src = (in_ref, gate_ref, outw_ref)[kind].at[
                layer, pl.ds(part * half, half), pl.ds(q * LANES, LANES)
            ]
            i, plane = 2 * zl + jnp.where(holder, 0, 1), 2 * hf + q // 2
        dst = segment(layer, kind, i, part)
        if local:
            return pltpu.make_async_copy(src, dst, wr.at[layer, kind, i])
        dev = {"sp": plane, "tp": 2 * c + q % 2}
        return remote(src, dst, ws.at[layer, kind], wr.at[layer, kind, i], dev)

    def weights_start(layer, kind):
        for q in range(T):
            chip = both(x == c, q // 2 == zl)
            if kind == MAPS:
                chip = both(chip, holder)

            @pl.when(jnp.logical_not(chip))
            def _():
                wcopy(layer, kind, q, g, False).start()

            @pl.when(both(chip, q % 2 == c))
            def _():
                for part in range(2):
                    wcopy(layer, kind, q, part, True).start()

            @pl.when(both(chip, q % 2 != c))
            def _():
                for part in range(2):
                    wcopy(layer, kind, q, part, False).start()

    def near(kind, i):
        if kind == MAPS:
            return both(holder, i == s)
        return i == 2 * zl + jnp.where(holder, 0, 1)

    def passing(layer, kind, i):
        at = segment(layer, kind, i, g)
        return remote(at, at, ys.at[layer, kind], yr.at[layer, kind], {"grp": 1 - g})

    def weights_forward(layer, kind):
        for i in range(4):

            @pl.when(jnp.logical_not(near(kind, i)))
            def _():
                bulk(segment(layer, kind, i, g), wr.at[layer, kind, i])
                passing(layer, kind, i).start()

    def passed(layer, kind, sem):
        deep = LANES if kind == MAPS else half
        if kind != MAPS:
            bulk(full.at[0, pl.ds(0, deep), pl.ds(0, 3 * LANES)], sem)
            return
        for n in (3, 4):

            @pl.when(holder if n == 3 else jnp.logical_not(holder))
            def _():
                bulk(full.at[0, pl.ds(0, deep), pl.ds(0, n * LANES)], sem)

    def weights_wait(layer, kind):
        for i in range(4):

            @pl.when(near(kind, i))
            def _():
                at = mbuf.at[layer, i] if kind == MAPS else wbuf.at[layer, kind, i // 2, :, :, lanes(i % 2)]
                bulk(at, wr.at[layer, kind, i])

        passed(layer, kind, yr.at[layer, kind])

    def weights_drain(layer, kind):
        deep = LANES if kind == MAPS else half
        bulk(full.at[0, pl.ds(0, deep), pl.ds(0, T * LANES)], ws.at[layer, kind])
        passed(layer, kind, ys.at[layer, kind])

    def piece_copy(b, dev, rsem, ssem):
        at = full.at[0, rows_at(b), piece]
        return remote(at, at, ssem, rsem, dev)

    def piece_z(b):
        return piece_copy(b, {"sp": sz}, ur.at[0, b, 0], us.at[0])

    def piece_x(b):
        return piece_copy(b, {"tp": tx}, ur.at[0, b, 0], us.at[1])

    def piece_c(b):
        return piece_copy(b, {"tp": tc}, cr.at[0, b], cs.at[0])

    def piece_far():
        return remote(tokb, full.at[0, rows_at(s), piece], us.at[1], ur.at[0, s, 0], {"sp": sp})

    def piece_arrive(i, b):
        @pl.when(jnp.logical_not(both(holder, i == 0)))
        def _():
            piece_z(b).wait_recv()

        @pl.when(i % 2 == 0)
        def _():
            piece_z(b).start()

            @pl.when(holder)
            def _():
                piece_x(b).start()

        piece_c(b).start()

    places = (
        ({"sp": sz}, T * x + 2 * (1 - zl) + c),
        ({"tp": tx}, T * (1 - x) + 2 * zl + c),
        ({"sp": sz, "tp": tx}, T * (1 - x) + 2 * (1 - zl) + c),
    )

    def unit_copy(gi, b, k):
        at = full.at[gi, rows_at(b), lanes(mine)]
        return remote(at, at, us.at[gi + 1], ur.at[gi, b, k], places[k][0])

    def unit_c(gi, b, j):
        at = full.at[gi, rows_at(b), lanes(j)]
        return remote(at, at, cs.at[gi], cr.at[gi, b], {"tp": tc})

    def unit_send(gi, b):
        for k in range(3):
            unit_copy(gi, b, k).start()
        unit_c(gi, b, mine).start()

    def unit_arrive(gi, b):
        for k in range(3):
            unit_copy(gi, b, k).wait_recv()
            unit_c(gi, b, places[k][1]).start()

    def across_wait(gi, b):
        bulk(full.at[gi, rows_at(b), pl.ds(0, T * LANES)], cr.at[gi, b])

    def part_copy(layer, kind, b):
        return remote(
            part.at[layer, kind, rows_at(b)],
            peer.at[layer, kind, rows_at(b)],
            ps.at[layer, kind],
            pr.at[layer, kind, b],
            {"sp": sp},
        )

    def partial(layer, kind, b, value, slot):
        prod = jnp.dot(
            value, wbuf[layer, kind].reshape(depth, 2 * LANES), preferred_element_type=F32
        )
        ownb[slot, rows_at(b), :] = prod[:, :LANES]
        part[layer, kind, rows_at(b), :] = prod[:, LANES:].astype(BF16)
        part_copy(layer, kind, b).start()

    def whole(layer, kind, b, slot):
        return ownb[slot, rows_at(b), :] + peer[layer, kind, rows_at(b), :].astype(F32)

    def row_of(column):
        return jnp.broadcast_to(column, (rows, LANES)).T[0:8]

    def column_of(row):
        return jnp.broadcast_to(row[0:1], (LANES, rows)).T

    def ssq_copy(layer):
        return remote(ssq.at[layer, 0], ssq.at[layer, 1], rs.at[layer], rr.at[layer], {"sp": sp})

    def block_at(layer, i):
        first = (jnp.where(i % 2 == 0, s, sz) + 2 * (i // 2)) % S
        return jnp.where(layer == 0, first, i)

    def in_phase(layer):
        gi = 2 * layer

        @pl.when(layer == 0)
        def _():
            @pl.loop(0, S)
            def _(i):
                piece_arrive(i, block_at(0, i))
                @pl.when(i == 1)
                def _():
                    weights_start(0, GATE)

                @pl.when(i == 2)
                def _():
                    weights_start(0, MAPS)
                    weights_forward(0, IN)

                @pl.when(i == 3)
                def _():
                    weights_forward(0, GATE)
                    weights_start(0, OUT)


        @pl.loop(0, S + 1)
        def _(i):
            @pl.when(both(layer > 0, i < S))
            def _():
                unit_arrive(gi, i)

            @pl.when(i == 1)
            def _():
                weights_wait(layer, IN)

            @pl.when(i > 0)
            def _():
                e = block_at(layer, i - 1)
                across_wait(gi, e)
                wide = full[gi, rows_at(e), :].astype(F32)
                ssq[layer, 0, e] = row_of(jnp.sum(wide * wide, axis=1, keepdims=True))
                gain = gain_ref[pl.ds(layer, 1), pl.ds(pl.multiple_of(hf * depth, depth), depth)]
                xg[rows_at(e), :] = (wide * gain).astype(BF16)
                partial(layer, IN, e, xg[rows_at(e), :], 0)

        ssq_copy(layer).start()
        weights_wait(layer, GATE)

        @pl.loop(0, S)
        def _(b):
            partial(layer, GATE, b, xg[rows_at(b), :], 1)

        weights_forward(layer, MAPS)

        @pl.when(layer + 1 < LAYERS)
        def _():
            weights_start(layer + 1, IN)
            weights_start(layer + 1, GATE)
            weights_start(layer + 1, MAPS)


        @pl.when(layer == 0)
        def _():
            params_wait()

        ssq_copy(layer).wait_recv()

        @pl.loop(0, S)
        def _(b):
            total = column_of(ssq[layer, 0, b] + ssq[layer, 1, b])
            scale = lax.rsqrt(total / D + EPS)
            scaleb[rows_at(b), :] = scale
            part_copy(layer, IN, b).wait_recv()
            xin = (scale * whole(layer, IN, b, 0)).astype(BF16).astype(F32)
            padded[pl.ds(pl.multiple_of(b * rows + 8, 8), rows), :] = xin

    def recurrence(layer):
        par = tapb[layer, :, lanes(sub)]
        rates = jax.nn.softplus(-logb[layer, :, lanes(sub)])
        edge = jnp.zeros((8, LANES), F32)
        padded[0:8, :] = edge
        padded[tokens + 8 : tokens + 16, :] = edge
        conv = par[0:1] * padded[6 : 6 + tokens, :]
        for k in range(1, TAPS):
            conv = conv + par[k : k + 1] * padded[6 + k : 6 + k + tokens, :]
        convb[layer, c] = conv.astype(BF16)
        vcopy = remote(
            convb.at[layer, c], convb.at[layer, c], vss.at[layer], vrs.at[layer], {"tp": tc}
        )
        vcopy.start()
        weights_wait(layer, MAPS)
        vcopy.wait()
        pair_in = jnp.concatenate([convb[layer, 0], convb[layer, 1]], axis=1)
        conv32 = convb[layer, c].astype(F32)
        hidden = None
        for d in range(2):
            pair = []
            for k in (2 * d, 2 * d + 1):
                pair.append(
                    jax.nn.sigmoid(jnp.dot(pair_in, mbuf[layer, k].reshape(HEAD_W, LANES), preferred_element_type=F32))
                )
            log_a = -8.0 * pair[0] * rates[d : d + 1]
            drive = jnp.sqrt(one_minus_exp_neg(-2.0 * log_a)) * pair[1] * conv32
            state = scan_rows(jnp.exp(log_a), drive, d == 1)
            hidden = state if hidden is None else hidden + state
        hid[...] = hidden
        weights_forward(layer, OUT)


        @pl.loop(0, S)
        def _(b):
            part_copy(layer, GATE, b).wait_recv()
            gin = (scaleb[rows_at(b), :] * whole(layer, GATE, b, 1)).astype(BF16).astype(F32)
            mix = (jax.nn.gelu(gin) * hid[rows_at(b), :]).astype(BF16)
            full[2 * layer + 1, rows_at(b), lanes(mine)] = mix
            unit_send(2 * layer + 1, b)

    def fcopy(b, local):
        src = last.at[rows_at(b)]
        dst = fin.at[:, lanes(sub)]
        if local:
            return pltpu.make_async_copy(src, dst, frs.at[0])
        return remote(src, dst, fss.at[b], frs.at[0], {"sp": b, "tp": block})

    def qcopy(b, dt):
        return remote(
            sfin.at[b], ssqf.at[T * s + t], qss.at[b, dt], qrs.at[0], {"sp": b, "tp": dt}
        )

    def final_here(b):
        return both(b == s, block == t)

    def final_send(b):
        @pl.when(final_here(b))
        def _():
            fcopy(b, True).start()

        @pl.when(jnp.logical_not(final_here(b)))
        def _():
            fcopy(b, False).start()

        for dt in range(T):

            @pl.when(both(b == s, t == dt))
            def _():
                ssqf[T * s + t] = sfin[b]

            @pl.when(jnp.logical_not(both(b == s, t == dt)))
            def _():
                qcopy(b, dt).start()

    def out_phase(layer):
        gi = 2 * layer + 1

        @pl.loop(0, S + 1)
        def _(i):
            @pl.when(i < S)
            def _():
                unit_arrive(gi, i)

            @pl.when(i == 1)
            def _():
                weights_wait(layer, OUT)

            @pl.when(i > 0)
            def _():
                across_wait(gi, i - 1)
                partial(layer, OUT, i - 1, full[gi, rows_at(i - 1), :], 0)

        @pl.when(layer + 1 < LAYERS)
        def _():
            weights_forward(layer + 1, IN)
            weights_forward(layer + 1, GATE)
            weights_start(layer + 1, OUT)


        @pl.loop(0, S)
        def _(b):
            part_copy(layer, OUT, b).wait_recv()
            old = full[gi - 1, rows_at(b), lanes(mine)].astype(F32)
            new = (old + whole(layer, OUT, b, 0)).astype(BF16)

            @pl.when(layer + 1 < LAYERS)
            def _():
                full[gi + 1, rows_at(b), lanes(mine)] = new
                unit_send(gi + 1, b)

            @pl.when(layer + 1 == LAYERS)
            def _():
                last[rows_at(b), :] = new
                wide = new.astype(F32)
                sfin[b] = row_of(jnp.sum(wide * wide, axis=1, keepdims=True))
                final_send(b)

    @pl.when(holder)
    def _():
        own_full.wait()

    @pl.when(jnp.logical_not(holder))
    def _():
        own_side.wait()
        piece_far().start()

    weights_start(0, IN)

    @pl.loop(0, LAYERS)
    def _(layer):
        in_phase(layer)
        recurrence(layer)
        out_phase(layer)

    bulk(ssqf.at[pl.ds(0, S * T - 1)], qrs.at[0])
    total = ssqf[0]
    for i in range(1, S * T):
        total = total + ssqf[i]
    total = column_of(total)[:, 0:1]
    bulk(fin, frs.at[0])
    out_ref[...] = (fin[...].astype(F32) * lax.rsqrt(total / D + EPS) * fgain_ref[...]).astype(BF16)

    for k in range(2):

        @pl.when(both(holder, 2 * c + k != t))
        def _():
            for copy in param_copies(k):
                copy.wait_send()

    for layer in range(LAYERS):
        for kind in range(4):
            weights_drain(layer, kind)
        for kind in range(3):
            bulk(part.at[layer, kind], ps.at[layer, kind])
        ssq_copy(layer).wait_send()
    bulk(full.at[0, pl.ds(0, 2 * rows), pl.ds(0, T * LANES)], us.at[0])

    @pl.when(holder)
    def _():
        bulk(full.at[0, pl.ds(0, 2 * rows), pl.ds(0, T * LANES)], us.at[1])

    @pl.when(jnp.logical_not(holder))
    def _():
        bulk(tokb, us.at[1])

    for gi in range(2 * LAYERS):
        bulk(full.at[gi, :, pl.ds(0, T * LANES)], cs.at[gi])
        if gi:
            bulk(full.at[gi, :, pl.ds(0, 3 * LANES)], us.at[gi + 1])
    for b in range(S):

        @pl.when(jnp.logical_not(final_here(b)))
        def _():
            fcopy(b, False).wait_send()

        for dt in range(T):

            @pl.when(jnp.logical_not(both(b == s, t == dt)))
            def _():
                qcopy(b, dt).wait_send()


def fused(mesh):
    S, T = mesh.shape["sp"], mesh.shape["tp"]

    def run(tokens, norm_gain, in_weight, gate_weight, conv_taps, decay_logit, gate_maps, out_weight, final_gain):
        rows, tcols = tokens.shape
        total = rows * S
        depth = D // 2
        dma = pltpu.SemaphoreType.DMA
        n = 2 * LAYERS
        vmem = pl.BlockSpec(memory_space=pltpu.VMEM)
        hbm = pl.BlockSpec(memory_space=pl.ANY)

        def body_of(*refs):
            kernel(S, T, *refs)

        return pl.pallas_call(
            body_of,
            out_shape=jax.ShapeDtypeStruct((rows, tcols), BF16),
            in_specs=[hbm, vmem, hbm, hbm, vmem, vmem, hbm, hbm, vmem],
            out_specs=vmem,
            scratch_shapes=[
                pltpu.VMEM((n, total, depth), BF16),
                pltpu.VMEM((rows, tcols), BF16),
                pltpu.VMEM((total, depth), BF16),
                pltpu.VMEM((LAYERS, 3, 2, 2, in_weight.shape[1] // 2, 2 * LANES), BF16),
                pltpu.VMEM((LAYERS, S, 2, LANES, LANES), BF16),
                pltpu.VMEM((LAYERS, TAPS, tcols), F32),
                pltpu.VMEM((LAYERS, 2, tcols), F32),
                pltpu.VMEM((2, total, LANES), F32),
                pltpu.VMEM((LAYERS, 3, total, LANES), BF16),
                pltpu.VMEM((LAYERS, 3, total, LANES), BF16),
                pltpu.VMEM((LAYERS, 2, S, 8, LANES), F32),
                pltpu.VMEM((total, LANES), F32),
                pltpu.VMEM((total + 16, LANES), F32),
                pltpu.VMEM((LAYERS, 2, total, LANES), BF16),
                pltpu.VMEM((total, LANES), F32),
                pltpu.VMEM((total, LANES), BF16),
                pltpu.VMEM((S, 8, LANES), F32),
                pltpu.VMEM((S * T, 8, LANES), F32),
                pltpu.VMEM((rows, tcols), BF16),
                dma((LAYERS, 4)),
                dma((LAYERS, 4, 4)),
                dma((LAYERS, 4)),
                dma((LAYERS, 4)),
                dma((n + 1,)),
                dma((n, S, 3)),
                dma((n,)),
                dma((n, S)),
                dma((LAYERS, 3)),
                dma((LAYERS, 3, S)),
                dma((LAYERS,)),
                dma((LAYERS,)),
                dma((LAYERS,)),
                dma((LAYERS,)),
                dma((2, 2)),
                dma((2,)),
                dma((S,)),
                dma((1,)),
                dma((S, T)),
                dma((1,)),
                dma((1,)),
            ],
            compiler_params=pltpu.CompilerParams(
                collective_id=0, has_side_effects=True, vmem_limit_bytes=60 * 1024 * 1024
            ),
        )(tokens, norm_gain, in_weight, gate_weight, conv_taps, decay_logit, gate_maps, out_weight, final_gain.reshape(1, tcols))

    return run


def solution(mesh):
    placed = (
        P(("grp", "sp"), "tp"),
        P(),
        P(None, "sp", "tp"),
        P(None, "sp", "tp"),
        P(None, None, "tp"),
        P(None, None, "tp"),
        P(None, "tp", "sp"),
        P(None, "sp", "tp"),
        P("tp"),
    )
    shape = dict(mesh.shape)
    fits = (
        shape["grp"] == 2
        and shape["tp"] == 4
        and shape["sp"] == 4
        and D == shape["sp"] * shape["tp"] * LANES
        and HEAD_W == 2 * LANES
    )
    return jax.shard_map(
        fused(mesh) if fits else body, mesh=mesh, in_specs=placed, out_specs=P(("grp", "sp"), "tp"), check_vma=False
    )
```

```python
import jax
import jax.numpy as jnp
from jax import lax
from jax.experimental import pallas as pl
from jax.experimental.pallas import tpu as pltpu
from jax.sharding import PartitionSpec as P

D = 2048
HEAD_W = 256
TAPS = 4
LAYERS = 2


EPS = 1e-06


def extended(value, sides, width):
    for axis, dim in sides:
        devices, length = (lax.axis_size(axis), value.shape[dim])
        up = [(i, (i + 1) % devices) for i in range(devices - 1)]
        down = [(j, i) for i, j in up]
        last = lax.slice_in_dim(value, length - width, length, axis=dim)
        leading = lax.slice_in_dim(value, 0, width, axis=dim)
        before = lax.ppermute(last, axis, up)
        after = lax.ppermute(leading, axis, down)
        value = jnp.concatenate([before, value, after], axis=dim)
    return value


def combine_pair(earlier, later):
    return (earlier[0] * later[0], later[0] * earlier[1] + later[1])


def body(
    tokens,
    norm_gain,
    in_weight,
    gate_weight,
    conv_taps,
    decay_logit,
    gate_maps,
    out_weight,
    final_gain,
):
    resid = tokens
    rows = tokens.shape[0]
    width = in_weight.shape[2]
    local_heads = width // HEAD_W
    for layer in range(LAYERS):
        whole = lax.all_gather(resid, "tp", axis=1, tiled=True)
        wide = whole.astype(jnp.float32)
        normed = (
            wide * lax.rsqrt(jnp.mean(wide * wide, axis=1, keepdims=True) + EPS) * norm_gain[layer]
        ).astype(jnp.bfloat16)
        proj_in = jnp.dot(
            normed,
            lax.all_gather(in_weight[layer], "sp", axis=0, tiled=True),
            preferred_element_type=jnp.float32,
        )
        proj_gate = jnp.dot(
            normed,
            lax.all_gather(gate_weight[layer], "sp", axis=0, tiled=True),
            preferred_element_type=jnp.float32,
        )
        xin = proj_in.astype(jnp.bfloat16)
        gin = proj_gate.astype(jnp.bfloat16)
        padded = extended(xin, (("sp", 0),), 2).astype(jnp.float32)
        conv = conv_taps[layer, 0] * padded[0:rows]
        for k in range(1, TAPS):
            conv = conv + conv_taps[layer, k] * padded[k : k + rows]
        conv = conv.astype(jnp.bfloat16)
        stacked = conv.reshape(rows, local_heads, HEAD_W)
        piece = lax.all_gather(gate_maps[layer], "sp", axis=1, tiled=True)
        blocks = piece.reshape(local_heads, HEAD_W, piece.shape[1])
        pre = jnp.einsum("thi,hij->thj", stacked, blocks, preferred_element_type=jnp.float32)
        pre = pre.reshape(rows, local_heads, 4, HEAD_W)
        conv32 = conv.astype(jnp.float32)
        locals_a = []
        locals_h = []
        for direction in range(2):
            rate = jax.nn.sigmoid(pre[:, :, 2 * direction]).reshape(rows, width)
            inp = jax.nn.sigmoid(pre[:, :, 2 * direction + 1]).reshape(rows, width)
            log_a = -8.0 * rate * jax.nn.softplus(-decay_logit[layer, direction])
            decay = jnp.exp(log_a)
            drive = jnp.sqrt(-jnp.expm1(2.0 * log_a)) * inp * conv32
            prod_a, state = lax.associative_scan(
                combine_pair, (decay, drive), reverse=direction == 1, axis=0
            )
            locals_a.append(prod_a)
            locals_h.append(state)
        summary = jnp.stack([locals_a[0][-1], locals_h[0][-1], locals_a[1][0], locals_h[1][0]])[
            None
        ]
        every = lax.all_gather(summary, "sp", axis=0, tiled=True)
        count = every.shape[0]
        me = lax.axis_index("sp")
        _, incl_f = lax.associative_scan(combine_pair, (every[:, 0], every[:, 1]), axis=0)
        _, incl_b = lax.associative_scan(
            combine_pair, (every[:, 2], every[:, 3]), reverse=True, axis=0
        )
        before = lax.dynamic_index_in_dim(incl_f, jnp.maximum(me - 1, 0), 0, keepdims=False)
        after = lax.dynamic_index_in_dim(incl_b, jnp.minimum(me + 1, count - 1), 0, keepdims=False)
        carry_f = before * (me > 0).astype(jnp.float32)
        carry_b = after * (me < count - 1).astype(jnp.float32)
        hidden = locals_h[0] + locals_a[0] * carry_f + locals_h[1] + locals_a[1] * carry_b
        mix = (jax.nn.gelu(gin.astype(jnp.float32)) * hidden).astype(jnp.bfloat16)
        full_mix = lax.all_gather(mix, "tp", axis=1, tiled=True)
        out = jnp.dot(
            full_mix,
            lax.all_gather(out_weight[layer], "sp", axis=0, tiled=True),
            preferred_element_type=jnp.float32,
        )
        resid = (resid.astype(jnp.float32) + out).astype(jnp.bfloat16)
    wide = resid.astype(jnp.float32)
    total = lax.psum(jnp.sum(wide * wide, axis=1), "tp")
    scale = lax.rsqrt(total / D + EPS)
    return (wide * scale[:, None] * final_gain).astype(jnp.bfloat16)


LANES = 128
IN, GATE, OUT, MAPS = range(4)
BF16 = jnp.bfloat16
F32 = jnp.float32


def shifted(value, k, fill, reverse):
    pad = jnp.full((k, value.shape[1]), fill, value.dtype)
    if reverse:
        return jnp.concatenate([value[k:], pad], axis=0)
    return jnp.concatenate([pad, value[:-k]], axis=0)


def scan_rows(decay, state, reverse):
    k, rows = 1, decay.shape[0]
    while k < rows:
        state = state + decay * shifted(state, k, 0.0, reverse)
        if 2 * k < rows:
            decay = decay * shifted(decay, k, 1.0, reverse)
        k *= 2
    return state


def one_minus_exp_neg(u):
    series = u * (1 - u / 2 * (1 - u / 3 * (1 - u / 4 * (1 - u / 5 * (1 - u / 6 * (1 - u / 7))))))
    return jnp.where(u < 0.3, series, 1.0 - jnp.exp(-u))


def kernel(
    S,
    T,
    tok_ref,
    gain_ref,
    in_ref,
    gate_ref,
    taps_ref,
    logit_ref,
    map_ref,
    outw_ref,
    fgain_ref,
    out_ref,
    full,
    tokb,
    xg,
    wbuf,
    mbuf,
    gainb,
    fgainb,
    tapb,
    logb,
    ownb,
    part,
    peer,
    ssq,
    scaleb,
    padded,
    convb,
    hid,
    last,
    sfin,
    ssqf,
    fin,
    ws,
    wr,
    ys,
    yr,
    us,
    ur,
    cs,
    cr,
    ps,
    pr,
    rs,
    rr,
    vss,
    vrs,
    pss,
    prs,
    fss,
    frs,
    qss,
    qrs,
    lsem,
):
    g = lax.axis_index("grp")
    s = lax.axis_index("sp")
    t = lax.axis_index("tp")
    x, c = t // 2, t % 2
    hf, zl = s // 2, s % 2
    sz = s + 1 - 2 * zl
    sp = (s + 2) % S
    tx = (t + 2) % T
    tc = t + 1 - 2 * c
    rows, tcols = tok_ref.shape
    tokens = rows * S
    depth = full.shape[2]
    block = 2 * hf + x
    sub = 2 * zl + c
    mine = T * x + sub
    holder = x == hf

    def lanes(i, n=1):
        return pl.ds(pl.multiple_of(i * LANES, LANES), n * LANES)

    def rows_at(b):
        return pl.ds(pl.multiple_of(b * rows, rows), rows)

    def remote(src, dst, ssem, rsem, dev):
        return pltpu.make_async_remote_copy(
            src_ref=src,
            dst_ref=dst,
            send_sem=ssem,
            recv_sem=rsem,
            device_id=dev,
            device_id_type=pl.DeviceIdType.MESH,
        )

    def bulk(ref, sem):
        pltpu.make_async_copy(ref, ref, sem).wait()

    def both(a, b):
        return jnp.logical_and(a, b)

    barrier = pltpu.get_barrier_semaphore()
    for ds in range(S):
        for dt in range(T):
            if ds or dt:
                pl.semaphore_signal(
                    barrier,
                    inc=1,
                    device_id={"sp": (s + ds) % S, "tp": (t + dt) % T},
                    device_id_type=pl.DeviceIdType.MESH,
                )

    pl.semaphore_signal(
        barrier, inc=1, device_id={"grp": 1 - g}, device_id_type=pl.DeviceIdType.MESH
    )

    piece = lanes(T * c, T)
    own_full = pltpu.make_async_copy(tok_ref, full.at[0, rows_at(s), piece], lsem.at[0])
    own_side = pltpu.make_async_copy(tok_ref, tokb, lsem.at[0])

    @pl.when(holder)
    def _():
        own_full.start()

    @pl.when(jnp.logical_not(holder))
    def _():
        own_side.start()

    gain_copy = pltpu.make_async_copy(
        gain_ref.at[:, pl.ds(pl.multiple_of(hf * depth, depth), depth)], gainb, lsem.at[1]
    )
    gain_copy.start()
    fgain_copy = pltpu.make_async_copy(fgain_ref, fgainb, lsem.at[2])
    fgain_copy.start()

    @pl.when(block == t)
    def _():
        pltpu.make_async_copy(taps_ref, tapb, prs.at[0]).start()
        pltpu.make_async_copy(logit_ref, logb, prs.at[1]).start()

    pl.semaphore_wait(barrier, S * T)

    def param_copies(k):
        dev = {"tp": 2 * c + k}
        return [
            remote(ref, buf, pss.at[i, k], prs.at[i], dev)
            for i, (ref, buf) in enumerate(((taps_ref, tapb), (logit_ref, logb)))
        ]

    for k in range(2):

        @pl.when(both(holder, 2 * c + k != t))
        def _():
            for copy in param_copies(k):
                copy.start()

    def params_wait():
        for copy in param_copies(0):
            copy.wait_recv()

    half = in_ref.shape[1] // 2

    def segment(layer, kind, i, part):
        if kind == MAPS:
            return mbuf.at[layer, i, part]
        return wbuf.at[layer, kind, i // 2, part, :, lanes(i % 2)]

    def wcopy(layer, kind, q, part, local):
        if kind == MAPS:
            src = map_ref.at[
                layer, pl.ds((q // 2) * HEAD_W + part * LANES, LANES), pl.ds((q % 2) * LANES, LANES)
            ]
            i, plane = s, 2 * x + q // 2
        else:
            src = (in_ref, gate_ref, outw_ref)[kind].at[
                layer, pl.ds(part * half, half), pl.ds(q * LANES, LANES)
            ]
            i, plane = 2 * zl + jnp.where(holder, 0, 1), 2 * hf + q // 2
        dst = segment(layer, kind, i, part)
        if local:
            return pltpu.make_async_copy(src, dst, wr.at[layer, kind, i])
        dev = {"sp": plane, "tp": 2 * c + q % 2}
        return remote(src, dst, ws.at[layer, kind], wr.at[layer, kind, i], dev)

    def weights_start(layer, kind):
        for q in range(T):
            chip = both(x == c, q // 2 == zl)
            if kind == MAPS:
                chip = both(chip, holder)

            @pl.when(jnp.logical_not(chip))
            def _():
                wcopy(layer, kind, q, g, False).start()

            @pl.when(both(chip, q % 2 == c))
            def _():
                for part in range(2):
                    wcopy(layer, kind, q, part, True).start()

            @pl.when(both(chip, q % 2 != c))
            def _():
                for part in range(2):
                    wcopy(layer, kind, q, part, False).start()

    def near(kind, i):
        if kind == MAPS:
            return both(holder, i == s)
        return i == 2 * zl + jnp.where(holder, 0, 1)

    def passing(layer, kind, i):
        at = segment(layer, kind, i, g)
        return remote(at, at, ys.at[layer, kind], yr.at[layer, kind], {"grp": 1 - g})

    def weights_forward(layer, kind):
        for i in range(4):

            @pl.when(jnp.logical_not(near(kind, i)))
            def _():
                bulk(segment(layer, kind, i, g), wr.at[layer, kind, i])
                passing(layer, kind, i).start()

    def passed(layer, kind, sem):
        deep = LANES if kind == MAPS else half
        if kind != MAPS:
            bulk(full.at[0, pl.ds(0, deep), pl.ds(0, 3 * LANES)], sem)
            return
        for n in (3, 4):

            @pl.when(holder if n == 3 else jnp.logical_not(holder))
            def _():
                bulk(full.at[0, pl.ds(0, deep), pl.ds(0, n * LANES)], sem)

    def weights_wait(layer, kind):
        for i in range(4):

            @pl.when(near(kind, i))
            def _():
                at = mbuf.at[layer, i] if kind == MAPS else wbuf.at[layer, kind, i // 2, :, :, lanes(i % 2)]
                bulk(at, wr.at[layer, kind, i])

        passed(layer, kind, yr.at[layer, kind])

    def weights_drain(layer, kind):
        deep = LANES if kind == MAPS else half
        bulk(full.at[0, pl.ds(0, deep), pl.ds(0, T * LANES)], ws.at[layer, kind])
        passed(layer, kind, ys.at[layer, kind])

    def piece_copy(b, dev, rsem, ssem):
        at = full.at[0, rows_at(b), piece]
        return remote(at, at, ssem, rsem, dev)

    def piece_z(b):
        return piece_copy(b, {"sp": sz}, ur.at[0, b, 0], us.at[0])

    def piece_x(b):
        return piece_copy(b, {"tp": tx}, ur.at[0, b, 0], us.at[1])

    def piece_c(b):
        return piece_copy(b, {"tp": tc}, cr.at[0, b], cs.at[0])

    hrows = rows // 2
    side = jnp.where(holder, 0, 1)

    def far_first(h):
        dev = {"sp": sp, "tp": tx} if h else {"sp": sp}
        return remote(
            tokb.at[pl.ds(h * hrows, hrows)],
            full.at[0, pl.ds(pl.multiple_of(s * rows + h * hrows, hrows), hrows), piece],
            us.at[1],
            ur.at[0, s, 0],
            dev,
        )

    def far_copy(b, h, k, dev):
        at = full.at[0, pl.ds(pl.multiple_of(b * rows + h * hrows, hrows), hrows), piece]
        if k is None:
            return remote(at, at, cs.at[0], cr.at[0, b], {"tp": tc})
        return remote(at, at, us.at[2 * LAYERS + 1], ur.at[0, b, k], dev)

    def far_arrive(b, h, k):
        far_copy(b, h, k, {"sp": sz}).wait_recv()
        far_copy(b, h, None, None).start()

    def pieces_arrive(hook):
        @pl.when(jnp.logical_not(holder))
        def _():
            piece_z(s).wait_recv()

        piece_z(s).start()

        @pl.when(holder)
        def _():
            piece_x(s).start()

        piece_c(s).start()
        hook(0)
        far_copy(sp, side, 0, {"sp": sz}).wait_recv()
        far_copy(sp, side, 1, {"sp": sz, "tp": tx}).start()
        far_copy(sp, side, 0, {"sp": sz}).start()
        far_copy(sp, side, 1, {"tp": tx}).start()
        far_copy(sp, side, None, None).start()
        hook(1)
        piece_z(sz).wait_recv()
        piece_c(sz).start()
        hook(2)
        far_arrive(sp, 1 - side, 1)
        far_arrive((sz + 2) % S, side, 0)
        far_arrive((sz + 2) % S, 1 - side, 1)
        hook(3)

    places = (
        ({"sp": sz}, T * x + 2 * (1 - zl) + c),
        ({"tp": tx}, T * (1 - x) + 2 * zl + c),
        ({"sp": sz, "tp": tx}, T * (1 - x) + 2 * (1 - zl) + c),
    )

    def unit_copy(gi, b, k):
        at = full.at[gi, rows_at(b), lanes(mine)]
        return remote(at, at, us.at[gi + 1], ur.at[gi, b, k], places[k][0])

    def unit_c(gi, b, j):
        at = full.at[gi, rows_at(b), lanes(j)]
        return remote(at, at, cs.at[gi], cr.at[gi, b], {"tp": tc})

    def unit_send(gi, b):
        for k in (2, 0, 1):
            unit_copy(gi, b, k).start()
        unit_c(gi, b, mine).start()

    def unit_arrive(gi, b):
        for k in range(3):
            unit_copy(gi, b, k).wait_recv()
            unit_c(gi, b, places[k][1]).start()

    def across_wait(gi, b):
        bulk(full.at[gi, rows_at(b), pl.ds(0, T * LANES)], cr.at[gi, b])

    def part_copy(layer, kind, b):
        return remote(
            part.at[layer, kind, rows_at(b)],
            peer.at[layer, kind, rows_at(b)],
            ps.at[layer, kind],
            pr.at[layer, kind, b],
            {"sp": sp},
        )

    def partial(layer, kind, b, value, slot):
        prod = jnp.dot(
            value, wbuf[layer, kind].reshape(depth, 2 * LANES), preferred_element_type=F32
        )
        ownb[slot, rows_at(b), :] = prod[:, :LANES]
        part[layer, kind, rows_at(b), :] = prod[:, LANES:].astype(BF16)
        part_copy(layer, kind, b).start()

    def whole(layer, kind, b, slot):
        return ownb[slot, rows_at(b), :] + peer[layer, kind, rows_at(b), :].astype(F32)

    def row_of(column):
        return jnp.broadcast_to(column, (rows, LANES)).T[0:8]

    def column_of(row):
        return jnp.broadcast_to(row[0:1], (LANES, rows)).T

    def ssq_copy(layer):
        return remote(ssq.at[layer, 0], ssq.at[layer, 1], rs.at[layer], rr.at[layer], {"sp": sp})

    def block_at(layer, i):
        first = (jnp.where(i % 2 == 0, s, sz) + 2 * (i // 2)) % S
        return jnp.where(layer == 0, first, i)

    def in_phase(layer):
        gi = 2 * layer

        @pl.when(layer == 0)
        def _():
            def hook(i):
                pass
                if i == 1:
                    weights_start(0, GATE)
                    weights_start(0, MAPS)
                if i == 2:
                    weights_forward(0, IN)
                    weights_start(0, OUT)
                if i == 3:
                    weights_forward(0, GATE)

            gain_copy.wait()
            pieces_arrive(hook)

        @pl.loop(0, S + 1)
        def _(i):
            @pl.when(both(layer > 0, i < S))
            def _():
                unit_arrive(gi, i)

            @pl.when(i == 1)
            def _():
                weights_wait(layer, IN)

            @pl.when(i > 0)
            def _():
                e = block_at(layer, i - 1)
                across_wait(gi, e)
                wide = full[gi, rows_at(e), :].astype(F32)
                ssq[layer, 0, e] = row_of(jnp.sum(wide * wide, axis=1, keepdims=True))
                gain = gainb[pl.ds(layer, 1), :]
                xg[rows_at(e), :] = (wide * gain).astype(BF16)
                partial(layer, IN, e, xg[rows_at(e), :], 0)

        ssq_copy(layer).start()
        @pl.when(layer == 1)
        def _():
            weights_start(layer, OUT)

        weights_wait(layer, GATE)

        @pl.loop(0, S)
        def _(b):
            partial(layer, GATE, b, xg[rows_at(b), :], 1)

        weights_forward(layer, MAPS)

        @pl.when(layer + 1 < LAYERS)
        def _():
            weights_start(layer + 1, IN)
            weights_start(layer + 1, GATE)
            weights_start(layer + 1, MAPS)


        @pl.when(layer == 0)
        def _():
            params_wait()

        ssq_copy(layer).wait_recv()

        @pl.loop(0, S)
        def _(b):
            total = column_of(ssq[layer, 0, b] + ssq[layer, 1, b])
            scale = lax.rsqrt(total / D + EPS)
            scaleb[rows_at(b), :] = scale
            part_copy(layer, IN, b).wait_recv()
            xin = (scale * whole(layer, IN, b, 0)).astype(BF16).astype(F32)
            padded[pl.ds(pl.multiple_of(b * rows + 8, 8), rows), :] = xin

    def recurrence(layer):
        par = tapb[layer, :, lanes(sub)]
        rates = jax.nn.softplus(-logb[layer, :, lanes(sub)])
        edge = jnp.zeros((8, LANES), F32)
        padded[0:8, :] = edge
        padded[tokens + 8 : tokens + 16, :] = edge
        conv = par[0:1] * padded[6 : 6 + tokens, :]
        for k in range(1, TAPS):
            conv = conv + par[k : k + 1] * padded[6 + k : 6 + k + tokens, :]
        convb[layer, c] = conv.astype(BF16)
        vcopy = remote(
            convb.at[layer, c], convb.at[layer, c], vss.at[layer], vrs.at[layer], {"tp": tc}
        )
        vcopy.start()
        weights_wait(layer, MAPS)
        vcopy.wait()
        pair_in = jnp.concatenate([convb[layer, 0], convb[layer, 1]], axis=1)
        conv32 = convb[layer, c].astype(F32)
        hidden = None
        for d in range(2):
            pair = []
            for k in (2 * d, 2 * d + 1):
                pair.append(
                    jax.nn.sigmoid(jnp.dot(pair_in, mbuf[layer, k].reshape(HEAD_W, LANES), preferred_element_type=F32))
                )
            log_a = -8.0 * pair[0] * rates[d : d + 1]
            drive = jnp.sqrt(one_minus_exp_neg(-2.0 * log_a)) * pair[1] * conv32
            state = scan_rows(jnp.exp(log_a), drive, d == 1)
            hidden = state if hidden is None else hidden + state
        hid[...] = hidden
        weights_forward(layer, OUT)


        @pl.loop(0, S)
        def _(b):
            part_copy(layer, GATE, b).wait_recv()
            gin = (scaleb[rows_at(b), :] * whole(layer, GATE, b, 1)).astype(BF16).astype(F32)
            mix = (jax.nn.gelu(gin) * hid[rows_at(b), :]).astype(BF16)
            full[2 * layer + 1, rows_at(b), lanes(mine)] = mix
            unit_send(2 * layer + 1, b)

    def fcopy(b, local):
        src = last.at[rows_at(b)]
        dst = fin.at[:, lanes(sub)]
        if local:
            return pltpu.make_async_copy(src, dst, frs.at[0])
        return remote(src, dst, fss.at[b], frs.at[0], {"sp": b, "tp": block})

    def qcopy(b, dt):
        return remote(
            sfin.at[b], ssqf.at[T * s + t], qss.at[b, dt], qrs.at[0], {"sp": b, "tp": dt}
        )

    def final_here(b):
        return both(b == s, block == t)

    def final_send(b):
        @pl.when(final_here(b))
        def _():
            fcopy(b, True).start()

        @pl.when(jnp.logical_not(final_here(b)))
        def _():
            fcopy(b, False).start()

        for dt in range(T):

            @pl.when(both(b == s, t == dt))
            def _():
                ssqf[T * s + t] = sfin[b]

            @pl.when(jnp.logical_not(both(b == s, t == dt)))
            def _():
                qcopy(b, dt).start()

    def out_phase(layer):
        gi = 2 * layer + 1

        @pl.loop(0, S + 1)
        def _(i):
            @pl.when(i < S)
            def _():
                unit_arrive(gi, i)

            @pl.when(i == 1)
            def _():
                weights_wait(layer, OUT)

            @pl.when(i > 0)
            def _():
                across_wait(gi, i - 1)
                partial(layer, OUT, i - 1, full[gi, rows_at(i - 1), :], 0)

        @pl.when(layer + 1 < LAYERS)
        def _():
            weights_forward(layer + 1, IN)
            weights_forward(layer + 1, GATE)


        @pl.loop(0, S)
        def _(b):
            part_copy(layer, OUT, b).wait_recv()
            old = full[gi - 1, rows_at(b), lanes(mine)].astype(F32)
            new = (old + whole(layer, OUT, b, 0)).astype(BF16)

            @pl.when(layer + 1 < LAYERS)
            def _():
                full[gi + 1, rows_at(b), lanes(mine)] = new
                unit_send(gi + 1, b)

            @pl.when(layer + 1 == LAYERS)
            def _():
                last[rows_at(b), :] = new
                wide = new.astype(F32)
                sfin[b] = row_of(jnp.sum(wide * wide, axis=1, keepdims=True))
                final_send(b)

    @pl.when(holder)
    def _():
        own_full.wait()

    @pl.when(jnp.logical_not(holder))
    def _():
        own_side.wait()
        for h in (1, 0):
            far_first(h).start()

    weights_start(0, IN)

    @pl.loop(0, LAYERS)
    def _(layer):
        in_phase(layer)
        recurrence(layer)
        out_phase(layer)

    bulk(ssqf.at[pl.ds(0, S * T - 1)], qrs.at[0])
    total = ssqf[0]
    for i in range(1, S * T):
        total = total + ssqf[i]
    total = column_of(total)[:, 0:1]
    bulk(fin, frs.at[0])
    fgain_copy.wait()
    out_ref[...] = (fin[...].astype(F32) * lax.rsqrt(total / D + EPS) * fgainb[...]).astype(BF16)

    for k in range(2):

        @pl.when(both(holder, 2 * c + k != t))
        def _():
            for copy in param_copies(k):
                copy.wait_send()

    for layer in range(LAYERS):
        for kind in range(4):
            weights_drain(layer, kind)
        for kind in range(3):
            bulk(part.at[layer, kind], ps.at[layer, kind])
        ssq_copy(layer).wait_send()
    for k in range(2):
        bulk(tokb, us.at[k])
    bulk(full.at[0, pl.ds(0, 3 * hrows), pl.ds(0, T * LANES)], us.at[2 * LAYERS + 1])
    for gi in range(2 * LAYERS):
        bulk(full.at[gi, :, pl.ds(0, T * LANES)], cs.at[gi])
        if gi:
            bulk(full.at[gi, :, pl.ds(0, 3 * LANES)], us.at[gi + 1])
    for b in range(S):

        @pl.when(jnp.logical_not(final_here(b)))
        def _():
            fcopy(b, False).wait_send()

        for dt in range(T):

            @pl.when(jnp.logical_not(both(b == s, t == dt)))
            def _():
                qcopy(b, dt).wait_send()


def fused(mesh):
    S, T = mesh.shape["sp"], mesh.shape["tp"]

    def run(tokens, norm_gain, in_weight, gate_weight, conv_taps, decay_logit, gate_maps, out_weight, final_gain):
        rows, tcols = tokens.shape
        total = rows * S
        depth = D // 2
        dma = pltpu.SemaphoreType.DMA
        n = 2 * LAYERS
        vmem = pl.BlockSpec(memory_space=pltpu.VMEM)
        hbm = pl.BlockSpec(memory_space=pl.ANY)

        def body_of(*refs):
            kernel(S, T, *refs)

        return pl.pallas_call(
            body_of,
            out_shape=jax.ShapeDtypeStruct((rows, tcols), BF16),
            in_specs=[hbm] * 9,
            out_specs=vmem,
            scratch_shapes=[
                pltpu.VMEM((n, total, depth), BF16),
                pltpu.VMEM((rows, tcols), BF16),
                pltpu.VMEM((total, depth), BF16),
                pltpu.VMEM((LAYERS, 3, 2, 2, in_weight.shape[1] // 2, 2 * LANES), BF16),
                pltpu.VMEM((LAYERS, S, 2, LANES, LANES), BF16),
                pltpu.VMEM((LAYERS, depth), F32),
                pltpu.VMEM((1, tcols), F32),
                pltpu.VMEM((LAYERS, TAPS, tcols), F32),
                pltpu.VMEM((LAYERS, 2, tcols), F32),
                pltpu.VMEM((2, total, LANES), F32),
                pltpu.VMEM((LAYERS, 3, total, LANES), BF16),
                pltpu.VMEM((LAYERS, 3, total, LANES), BF16),
                pltpu.VMEM((LAYERS, 2, S, 8, LANES), F32),
                pltpu.VMEM((total, LANES), F32),
                pltpu.VMEM((total + 16, LANES), F32),
                pltpu.VMEM((LAYERS, 2, total, LANES), BF16),
                pltpu.VMEM((total, LANES), F32),
                pltpu.VMEM((total, LANES), BF16),
                pltpu.VMEM((S, 8, LANES), F32),
                pltpu.VMEM((S * T, 8, LANES), F32),
                pltpu.VMEM((rows, tcols), BF16),
                dma((LAYERS, 4)),
                dma((LAYERS, 4, 4)),
                dma((LAYERS, 4)),
                dma((LAYERS, 4)),
                dma((n + 2,)),
                dma((n, S, 3)),
                dma((n,)),
                dma((n, S)),
                dma((LAYERS, 3)),
                dma((LAYERS, 3, S)),
                dma((LAYERS,)),
                dma((LAYERS,)),
                dma((LAYERS,)),
                dma((LAYERS,)),
                dma((2, 2)),
                dma((2,)),
                dma((S,)),
                dma((1,)),
                dma((S, T)),
                dma((1,)),
                dma((3,)),
            ],
            compiler_params=pltpu.CompilerParams(
                collective_id=0, has_side_effects=True, vmem_limit_bytes=60 * 1024 * 1024
            ),
        )(tokens, norm_gain, in_weight, gate_weight, conv_taps, decay_logit, gate_maps, out_weight, final_gain.reshape(1, tcols))

    return run


def solution(mesh):
    placed = (
        P(("grp", "sp"), "tp"),
        P(),
        P(None, "sp", "tp"),
        P(None, "sp", "tp"),
        P(None, None, "tp"),
        P(None, None, "tp"),
        P(None, "tp", "sp"),
        P(None, "sp", "tp"),
        P("tp"),
    )
    shape = dict(mesh.shape)
    fits = (
        shape["grp"] == 2
        and shape["tp"] == 4
        and shape["sp"] == 4
        and D == shape["sp"] * shape["tp"] * LANES
        and HEAD_W == 2 * LANES
    )
    return jax.shard_map(
        fused(mesh) if fits else body, mesh=mesh, in_specs=placed, out_specs=P(("grp", "sp"), "tp"), check_vma=False
    )
```

```python
import jax
import jax.numpy as jnp
from jax import lax
from jax.experimental import pallas as pl
from jax.experimental.pallas import tpu as pltpu
from jax.sharding import PartitionSpec as P

D = 2048
HEAD_W = 256
TAPS = 4
LAYERS = 2


EPS = 1e-06


def extended(value, sides, width):
    for axis, dim in sides:
        devices, length = (lax.axis_size(axis), value.shape[dim])
        up = [(i, (i + 1) % devices) for i in range(devices - 1)]
        down = [(j, i) for i, j in up]
        last = lax.slice_in_dim(value, length - width, length, axis=dim)
        leading = lax.slice_in_dim(value, 0, width, axis=dim)
        before = lax.ppermute(last, axis, up)
        after = lax.ppermute(leading, axis, down)
        value = jnp.concatenate([before, value, after], axis=dim)
    return value


def combine_pair(earlier, later):
    return (earlier[0] * later[0], later[0] * earlier[1] + later[1])


def body(
    tokens,
    norm_gain,
    in_weight,
    gate_weight,
    conv_taps,
    decay_logit,
    gate_maps,
    out_weight,
    final_gain,
):
    resid = tokens
    rows = tokens.shape[0]
    width = in_weight.shape[2]
    local_heads = width // HEAD_W
    for layer in range(LAYERS):
        whole = lax.all_gather(resid, "tp", axis=1, tiled=True)
        wide = whole.astype(jnp.float32)
        normed = (
            wide * lax.rsqrt(jnp.mean(wide * wide, axis=1, keepdims=True) + EPS) * norm_gain[layer]
        ).astype(jnp.bfloat16)
        proj_in = jnp.dot(
            normed,
            lax.all_gather(in_weight[layer], "sp", axis=0, tiled=True),
            preferred_element_type=jnp.float32,
        )
        proj_gate = jnp.dot(
            normed,
            lax.all_gather(gate_weight[layer], "sp", axis=0, tiled=True),
            preferred_element_type=jnp.float32,
        )
        xin = proj_in.astype(jnp.bfloat16)
        gin = proj_gate.astype(jnp.bfloat16)
        padded = extended(xin, (("sp", 0),), 2).astype(jnp.float32)
        conv = conv_taps[layer, 0] * padded[0:rows]
        for k in range(1, TAPS):
            conv = conv + conv_taps[layer, k] * padded[k : k + rows]
        conv = conv.astype(jnp.bfloat16)
        stacked = conv.reshape(rows, local_heads, HEAD_W)
        piece = lax.all_gather(gate_maps[layer], "sp", axis=1, tiled=True)
        blocks = piece.reshape(local_heads, HEAD_W, piece.shape[1])
        pre = jnp.einsum("thi,hij->thj", stacked, blocks, preferred_element_type=jnp.float32)
        pre = pre.reshape(rows, local_heads, 4, HEAD_W)
        conv32 = conv.astype(jnp.float32)
        locals_a = []
        locals_h = []
        for direction in range(2):
            rate = jax.nn.sigmoid(pre[:, :, 2 * direction]).reshape(rows, width)
            inp = jax.nn.sigmoid(pre[:, :, 2 * direction + 1]).reshape(rows, width)
            log_a = -8.0 * rate * jax.nn.softplus(-decay_logit[layer, direction])
            decay = jnp.exp(log_a)
            drive = jnp.sqrt(-jnp.expm1(2.0 * log_a)) * inp * conv32
            prod_a, state = lax.associative_scan(
                combine_pair, (decay, drive), reverse=direction == 1, axis=0
            )
            locals_a.append(prod_a)
            locals_h.append(state)
        summary = jnp.stack([locals_a[0][-1], locals_h[0][-1], locals_a[1][0], locals_h[1][0]])[
            None
        ]
        every = lax.all_gather(summary, "sp", axis=0, tiled=True)
        count = every.shape[0]
        me = lax.axis_index("sp")
        _, incl_f = lax.associative_scan(combine_pair, (every[:, 0], every[:, 1]), axis=0)
        _, incl_b = lax.associative_scan(
            combine_pair, (every[:, 2], every[:, 3]), reverse=True, axis=0
        )
        before = lax.dynamic_index_in_dim(incl_f, jnp.maximum(me - 1, 0), 0, keepdims=False)
        after = lax.dynamic_index_in_dim(incl_b, jnp.minimum(me + 1, count - 1), 0, keepdims=False)
        carry_f = before * (me > 0).astype(jnp.float32)
        carry_b = after * (me < count - 1).astype(jnp.float32)
        hidden = locals_h[0] + locals_a[0] * carry_f + locals_h[1] + locals_a[1] * carry_b
        mix = (jax.nn.gelu(gin.astype(jnp.float32)) * hidden).astype(jnp.bfloat16)
        full_mix = lax.all_gather(mix, "tp", axis=1, tiled=True)
        out = jnp.dot(
            full_mix,
            lax.all_gather(out_weight[layer], "sp", axis=0, tiled=True),
            preferred_element_type=jnp.float32,
        )
        resid = (resid.astype(jnp.float32) + out).astype(jnp.bfloat16)
    wide = resid.astype(jnp.float32)
    total = lax.psum(jnp.sum(wide * wide, axis=1), "tp")
    scale = lax.rsqrt(total / D + EPS)
    return (wide * scale[:, None] * final_gain).astype(jnp.bfloat16)


LANES = 128
IN, GATE, OUT, MAPS = range(4)
BF16 = jnp.bfloat16
F32 = jnp.float32


def shifted(value, k, fill, reverse):
    pad = jnp.full((k, value.shape[1]), fill, value.dtype)
    if reverse:
        return jnp.concatenate([value[k:], pad], axis=0)
    return jnp.concatenate([pad, value[:-k]], axis=0)


def scan_rows(decay, state, reverse):
    k, rows = 1, decay.shape[0]
    while k < rows:
        state = state + decay * shifted(state, k, 0.0, reverse)
        if 2 * k < rows:
            decay = decay * shifted(decay, k, 1.0, reverse)
        k *= 2
    return state


def sigmoid(v):
    return 0.5 * jnp.tanh(0.5 * v) + 0.5


def one_minus_square(u, decay):
    series = u * (1 - u / 2 * (1 - u / 3 * (1 - u / 4 * (1 - u / 5 * (1 - u / 6 * (1 - u / 7))))))
    return jnp.where(u < 0.3, series, 1.0 - decay * decay)


def kernel(
    S,
    T,
    tok_ref,
    gain_ref,
    in_ref,
    gate_ref,
    taps_ref,
    logit_ref,
    map_ref,
    outw_ref,
    fgain_ref,
    out_ref,
    full,
    tokb,
    xg,
    wbuf,
    mbuf,
    gainb,
    fgainb,
    tapb,
    logb,
    ownb,
    part,
    peer,
    ssq,
    scaleb,
    padded,
    convb,
    hid,
    last,
    sfin,
    ssqf,
    fin,
    ws,
    wr,
    ys,
    yr,
    us,
    ur,
    cs,
    cr,
    ps,
    pr,
    rs,
    rr,
    vss,
    vrs,
    pss,
    prs,
    fss,
    frs,
    qss,
    qrs,
    lsem,
):
    g = lax.axis_index("grp")
    s = lax.axis_index("sp")
    t = lax.axis_index("tp")
    x, c = t // 2, t % 2
    hf, zl = s // 2, s % 2
    sz = s + 1 - 2 * zl
    sp = (s + 2) % S
    tx = (t + 2) % T
    tc = t + 1 - 2 * c
    rows, tcols = tok_ref.shape
    tokens = rows * S
    depth = full.shape[2]
    block = 2 * hf + x
    sub = 2 * zl + c
    mine = T * x + sub
    holder = x == hf

    def lanes(i, n=1):
        return pl.ds(pl.multiple_of(i * LANES, LANES), n * LANES)

    def rows_at(b):
        return pl.ds(pl.multiple_of(b * rows, rows), rows)

    def remote(src, dst, ssem, rsem, dev):
        return pltpu.make_async_remote_copy(
            src_ref=src,
            dst_ref=dst,
            send_sem=ssem,
            recv_sem=rsem,
            device_id=dev,
            device_id_type=pl.DeviceIdType.MESH,
        )

    def bulk(ref, sem):
        pltpu.make_async_copy(ref, ref, sem).wait()

    def both(a, b):
        return jnp.logical_and(a, b)

    barrier = pltpu.get_barrier_semaphore()
    for ds in range(S):
        for dt in range(T):
            if ds or dt:
                pl.semaphore_signal(
                    barrier,
                    inc=1,
                    device_id={"sp": (s + ds) % S, "tp": (t + dt) % T},
                    device_id_type=pl.DeviceIdType.MESH,
                )

    pl.semaphore_signal(
        barrier, inc=1, device_id={"grp": 1 - g}, device_id_type=pl.DeviceIdType.MESH
    )

    piece = lanes(T * c, T)
    own_full = pltpu.make_async_copy(tok_ref, full.at[0, rows_at(s), piece], lsem.at[0])
    own_side = pltpu.make_async_copy(tok_ref, tokb, lsem.at[0])

    @pl.when(holder)
    def _():
        own_full.start()

    @pl.when(jnp.logical_not(holder))
    def _():
        own_side.start()

    gain_copy = pltpu.make_async_copy(
        gain_ref.at[:, pl.ds(pl.multiple_of(hf * depth, depth), depth)], gainb, lsem.at[1]
    )
    gain_copy.start()
    fgain_copy = pltpu.make_async_copy(fgain_ref, fgainb, lsem.at[2])
    fgain_copy.start()

    @pl.when(block == t)
    def _():
        pltpu.make_async_copy(taps_ref, tapb, prs.at[0]).start()
        pltpu.make_async_copy(logit_ref, logb, prs.at[1]).start()

    pl.semaphore_wait(barrier, S * T)

    def param_copies(k):
        dev = {"tp": 2 * c + k}
        return [
            remote(ref, buf, pss.at[i, k], prs.at[i], dev)
            for i, (ref, buf) in enumerate(((taps_ref, tapb), (logit_ref, logb)))
        ]

    for k in range(2):

        @pl.when(both(holder, 2 * c + k != t))
        def _():
            for copy in param_copies(k):
                copy.start()

    def params_wait():
        for copy in param_copies(0):
            copy.wait_recv()

    half = in_ref.shape[1] // 2

    def segment(layer, kind, i, part):
        if kind == MAPS:
            return mbuf.at[layer, i, part]
        return wbuf.at[layer, kind, i // 2, part, :, lanes(i % 2)]

    def wcopy(layer, kind, q, part, local):
        if kind == MAPS:
            src = map_ref.at[
                layer, pl.ds((q // 2) * HEAD_W + part * LANES, LANES), pl.ds((q % 2) * LANES, LANES)
            ]
            i, plane = s, 2 * x + q // 2
        else:
            src = (in_ref, gate_ref, outw_ref)[kind].at[
                layer, pl.ds(part * half, half), pl.ds(q * LANES, LANES)
            ]
            i, plane = 2 * zl + jnp.where(holder, 0, 1), 2 * hf + q // 2
        dst = segment(layer, kind, i, part)
        if local:
            return pltpu.make_async_copy(src, dst, wr.at[layer, kind, i])
        dev = {"sp": plane, "tp": 2 * c + q % 2}
        return remote(src, dst, ws.at[layer, kind], wr.at[layer, kind, i], dev)

    def weights_start(layer, kind):
        for q in range(T):
            chip = both(x == c, q // 2 == zl)
            if kind == MAPS:
                chip = both(chip, holder)

            @pl.when(jnp.logical_not(chip))
            def _():
                wcopy(layer, kind, q, g, False).start()

            @pl.when(both(chip, q % 2 == c))
            def _():
                for part in range(2):
                    wcopy(layer, kind, q, part, True).start()

            @pl.when(both(chip, q % 2 != c))
            def _():
                for part in range(2):
                    wcopy(layer, kind, q, part, False).start()

    def near(kind, i):
        if kind == MAPS:
            return both(holder, i == s)
        return i == 2 * zl + jnp.where(holder, 0, 1)

    def passing(layer, kind, i):
        at = segment(layer, kind, i, g)
        return remote(at, at, ys.at[layer, kind], yr.at[layer, kind], {"grp": 1 - g})

    def weights_forward(layer, kind):
        for i in range(4):

            @pl.when(jnp.logical_not(near(kind, i)))
            def _():
                bulk(segment(layer, kind, i, g), wr.at[layer, kind, i])
                passing(layer, kind, i).start()

    def passed(layer, kind, sem):
        deep = LANES if kind == MAPS else half
        if kind != MAPS:
            bulk(full.at[0, pl.ds(0, deep), pl.ds(0, 3 * LANES)], sem)
            return
        for n in (3, 4):

            @pl.when(holder if n == 3 else jnp.logical_not(holder))
            def _():
                bulk(full.at[0, pl.ds(0, deep), pl.ds(0, n * LANES)], sem)

    def weights_wait(layer, kind):
        for i in range(4):

            @pl.when(near(kind, i))
            def _():
                at = mbuf.at[layer, i] if kind == MAPS else wbuf.at[layer, kind, i // 2, :, :, lanes(i % 2)]
                bulk(at, wr.at[layer, kind, i])

        passed(layer, kind, yr.at[layer, kind])

    def weights_drain(layer, kind):
        deep = LANES if kind == MAPS else half
        bulk(full.at[0, pl.ds(0, deep), pl.ds(0, T * LANES)], ws.at[layer, kind])
        passed(layer, kind, ys.at[layer, kind])

    def piece_copy(b, dev, rsem, ssem):
        at = full.at[0, rows_at(b), piece]
        return remote(at, at, ssem, rsem, dev)

    def piece_z(b):
        return piece_copy(b, {"sp": sz}, ur.at[0, b, 0], us.at[0])

    def piece_x(b):
        return piece_copy(b, {"tp": tx}, ur.at[0, b, 0], us.at[1])

    def piece_c(b):
        return piece_copy(b, {"tp": tc}, cr.at[0, b], cs.at[0])

    hrows = rows // 2
    side = jnp.where(holder, 0, 1)

    def far_first(h):
        dev = {"sp": sp, "tp": tx} if h else {"sp": sp}
        return remote(
            tokb.at[pl.ds(h * hrows, hrows)],
            full.at[0, pl.ds(pl.multiple_of(s * rows + h * hrows, hrows), hrows), piece],
            us.at[1],
            ur.at[0, s, 0],
            dev,
        )

    def far_copy(b, h, k, dev):
        at = full.at[0, pl.ds(pl.multiple_of(b * rows + h * hrows, hrows), hrows), piece]
        if k is None:
            return remote(at, at, cs.at[0], cr.at[0, b], {"tp": tc})
        return remote(at, at, us.at[2 * LAYERS + 1], ur.at[0, b, k], dev)

    def far_arrive(b, h, k):
        far_copy(b, h, k, {"sp": sz}).wait_recv()
        far_copy(b, h, None, None).start()

    def pieces_arrive(hook):
        @pl.when(jnp.logical_not(holder))
        def _():
            piece_z(s).wait_recv()

        piece_z(s).start()

        @pl.when(holder)
        def _():
            piece_x(s).start()

        piece_c(s).start()
        hook(0)
        far_copy(sp, side, 0, {"sp": sz}).wait_recv()
        far_copy(sp, side, 1, {"sp": sz, "tp": tx}).start()
        far_copy(sp, side, 0, {"sp": sz}).start()
        far_copy(sp, side, 1, {"tp": tx}).start()
        far_copy(sp, side, None, None).start()
        hook(1)
        piece_z(sz).wait_recv()
        piece_c(sz).start()
        hook(2)
        far_arrive(sp, 1 - side, 1)
        far_arrive((sz + 2) % S, side, 0)
        far_arrive((sz + 2) % S, 1 - side, 1)
        hook(3)

    places = (
        ({"sp": sz}, T * x + 2 * (1 - zl) + c),
        ({"tp": tx}, T * (1 - x) + 2 * zl + c),
        ({"sp": sz, "tp": tx}, T * (1 - x) + 2 * (1 - zl) + c),
    )

    def unit_copy(gi, b, k):
        at = full.at[gi, rows_at(b), lanes(mine)]
        return remote(at, at, us.at[gi + 1], ur.at[gi, b, k], places[k][0])

    def unit_c(gi, b, j):
        at = full.at[gi, rows_at(b), lanes(j)]
        return remote(at, at, cs.at[gi], cr.at[gi, b], {"tp": tc})

    def unit_send(gi, b):
        for k in (2, 0, 1):
            unit_copy(gi, b, k).start()
        unit_c(gi, b, mine).start()

    def unit_arrive(gi, b):
        for k in range(3):
            unit_copy(gi, b, k).wait_recv()
            unit_c(gi, b, places[k][1]).start()

    def across_wait(gi, b):
        bulk(full.at[gi, rows_at(b), pl.ds(0, T * LANES)], cr.at[gi, b])

    def part_copy(layer, kind, b):
        return remote(
            part.at[layer, kind, rows_at(b)],
            peer.at[layer, kind, rows_at(b)],
            ps.at[layer, kind],
            pr.at[layer, kind, b],
            {"sp": sp},
        )

    def partial(layer, kind, b, value, slot):
        prod = jnp.dot(
            value, wbuf[layer, kind].reshape(depth, 2 * LANES), preferred_element_type=F32
        )
        ownb[slot, rows_at(b), :] = prod[:, :LANES]
        part[layer, kind, rows_at(b), :] = prod[:, LANES:].astype(BF16)
        part_copy(layer, kind, b).start()

    def whole(layer, kind, b, slot):
        return ownb[slot, rows_at(b), :] + peer[layer, kind, rows_at(b), :].astype(F32)

    def row_of(column):
        return jnp.broadcast_to(column, (rows, LANES)).T[0:8]

    def column_of(row):
        return jnp.broadcast_to(row[0:1], (LANES, rows)).T

    def ssq_copy(layer):
        return remote(ssq.at[layer, 0], ssq.at[layer, 1], rs.at[layer], rr.at[layer], {"sp": sp})

    def block_at(layer, i):
        first = (jnp.where(i % 2 == 0, s, sz) + 2 * (i // 2)) % S
        return jnp.where(layer == 0, first, i)

    def in_phase(layer):
        gi = 2 * layer

        @pl.when(layer == 0)
        def _():
            def hook(i):
                pass
                if i == 1:
                    weights_start(0, GATE)
                    weights_start(0, MAPS)
                if i == 2:
                    weights_forward(0, IN)
                    weights_start(0, OUT)
                if i == 3:
                    weights_forward(0, GATE)

            gain_copy.wait()
            pieces_arrive(hook)

        @pl.loop(0, S + 1)
        def _(i):
            @pl.when(both(layer > 0, i < S))
            def _():
                unit_arrive(gi, i)

            @pl.when(i == 1)
            def _():
                weights_wait(layer, IN)

            @pl.when(i > 0)
            def _():
                e = block_at(layer, i - 1)
                across_wait(gi, e)
                wide = full[gi, rows_at(e), :].astype(F32)
                gain = gainb[pl.ds(layer, 1), :]
                xg[rows_at(e), :] = (wide * gain).astype(BF16)
                partial(layer, IN, e, xg[rows_at(e), :], 0)
                ssq[layer, 0, e] = row_of(jnp.sum(wide * wide, axis=1, keepdims=True))

        ssq_copy(layer).start()
        @pl.when(layer == 1)
        def _():
            weights_start(layer, OUT)

        weights_wait(layer, GATE)

        @pl.loop(0, S)
        def _(b):
            partial(layer, GATE, b, xg[rows_at(b), :], 1)

        weights_forward(layer, MAPS)

        @pl.when(layer + 1 < LAYERS)
        def _():
            weights_start(layer + 1, IN)
            weights_start(layer + 1, GATE)
            weights_start(layer + 1, MAPS)

        @pl.when(layer == 0)
        def _():
            weights_forward(0, OUT)


        @pl.when(layer == 0)
        def _():
            params_wait()

        ssq_copy(layer).wait_recv()

        @pl.loop(0, S)
        def _(b):
            total = column_of(ssq[layer, 0, b] + ssq[layer, 1, b])
            scale = lax.rsqrt(total / D + EPS)
            scaleb[rows_at(b), :] = scale
            part_copy(layer, IN, b).wait_recv()
            xin = (scale * whole(layer, IN, b, 0)).astype(BF16).astype(F32)
            padded[pl.ds(pl.multiple_of(b * rows + 8, 8), rows), :] = xin

    def recurrence(layer):
        par = tapb[layer, :, lanes(sub)]
        rates = jax.nn.softplus(-logb[layer, :, lanes(sub)])
        edge = jnp.zeros((8, LANES), F32)
        padded[0:8, :] = edge
        padded[tokens + 8 : tokens + 16, :] = edge
        conv = par[0:1] * padded[6 : 6 + tokens, :]
        for k in range(1, TAPS):
            conv = conv + par[k : k + 1] * padded[6 + k : 6 + k + tokens, :]
        convb[layer, c] = conv.astype(BF16)
        vcopy = remote(
            convb.at[layer, c], convb.at[layer, c], vss.at[layer], vrs.at[layer], {"tp": tc}
        )
        vcopy.start()
        weights_wait(layer, MAPS)
        vcopy.wait()
        pair_in = jnp.concatenate([convb[layer, 0], convb[layer, 1]], axis=1)
        conv32 = convb[layer, c].astype(F32)
        hidden = None
        for d in range(2):
            pair = []
            for k in (2 * d, 2 * d + 1):
                pair.append(
                    sigmoid(jnp.dot(pair_in, mbuf[layer, k].reshape(HEAD_W, LANES), preferred_element_type=F32))
                )
            log_a = -8.0 * pair[0] * rates[d : d + 1]
            decay = jnp.exp(log_a)
            drive = jnp.sqrt(one_minus_square(-2.0 * log_a, decay)) * pair[1] * conv32
            state = scan_rows(decay, drive, d == 1)
            hidden = state if hidden is None else hidden + state
        hid[...] = hidden
        @pl.when(layer == 1)
        def _():
            weights_forward(1, OUT)


        @pl.loop(0, S)
        def _(b):
            part_copy(layer, GATE, b).wait_recv()
            gin = (scaleb[rows_at(b), :] * whole(layer, GATE, b, 1)).astype(BF16).astype(F32)
            mix = (jax.nn.gelu(gin) * hid[rows_at(b), :]).astype(BF16)
            full[2 * layer + 1, rows_at(b), lanes(mine)] = mix
            unit_send(2 * layer + 1, b)

    def fcopy(b, local):
        src = last.at[rows_at(b)]
        dst = fin.at[:, lanes(sub)]
        if local:
            return pltpu.make_async_copy(src, dst, frs.at[0])
        return remote(src, dst, fss.at[b], frs.at[0], {"sp": b, "tp": block})

    def qcopy(b, dt):
        return remote(
            sfin.at[b], ssqf.at[T * s + t], qss.at[b, dt], qrs.at[0], {"sp": b, "tp": dt}
        )

    def final_here(b):
        return both(b == s, block == t)

    def final_send(b):
        @pl.when(final_here(b))
        def _():
            fcopy(b, True).start()

        @pl.when(jnp.logical_not(final_here(b)))
        def _():
            fcopy(b, False).start()

        for dt in range(T):

            @pl.when(both(b == s, t == dt))
            def _():
                ssqf[T * s + t] = sfin[b]

            @pl.when(jnp.logical_not(both(b == s, t == dt)))
            def _():
                qcopy(b, dt).start()

    def out_phase(layer):
        gi = 2 * layer + 1

        @pl.loop(0, S + 1)
        def _(i):
            @pl.when(i < S)
            def _():
                unit_arrive(gi, i)

            @pl.when(i == 1)
            def _():
                weights_wait(layer, OUT)

            @pl.when(i > 0)
            def _():
                across_wait(gi, i - 1)
                partial(layer, OUT, i - 1, full[gi, rows_at(i - 1), :], 0)

        @pl.when(layer + 1 < LAYERS)
        def _():
            weights_forward(layer + 1, IN)
            weights_forward(layer + 1, GATE)


        @pl.loop(0, S)
        def _(b):
            part_copy(layer, OUT, b).wait_recv()
            old = full[gi - 1, rows_at(b), lanes(mine)].astype(F32)
            new = (old + whole(layer, OUT, b, 0)).astype(BF16)

            @pl.when(layer + 1 < LAYERS)
            def _():
                full[gi + 1, rows_at(b), lanes(mine)] = new
                unit_send(gi + 1, b)

            @pl.when(layer + 1 == LAYERS)
            def _():
                last[rows_at(b), :] = new
                wide = new.astype(F32)
                sfin[b] = row_of(jnp.sum(wide * wide, axis=1, keepdims=True))
                final_send(b)

    @pl.when(holder)
    def _():
        own_full.wait()

    @pl.when(jnp.logical_not(holder))
    def _():
        own_side.wait()
        for h in (1, 0):
            far_first(h).start()

    weights_start(0, IN)

    @pl.loop(0, LAYERS)
    def _(layer):
        in_phase(layer)
        recurrence(layer)
        out_phase(layer)

    bulk(ssqf.at[pl.ds(0, S * T - 1)], qrs.at[0])
    total = ssqf[0]
    for i in range(1, S * T):
        total = total + ssqf[i]
    total = column_of(total)[:, 0:1]
    bulk(fin, frs.at[0])
    fgain_copy.wait()
    out_ref[...] = (fin[...].astype(F32) * lax.rsqrt(total / D + EPS) * fgainb[...]).astype(BF16)

    for k in range(2):

        @pl.when(both(holder, 2 * c + k != t))
        def _():
            for copy in param_copies(k):
                copy.wait_send()

    for layer in range(LAYERS):
        for kind in range(4):
            weights_drain(layer, kind)
        for kind in range(3):
            bulk(part.at[layer, kind], ps.at[layer, kind])
        ssq_copy(layer).wait_send()
    for k in range(2):
        bulk(tokb, us.at[k])
    bulk(full.at[0, pl.ds(0, 3 * hrows), pl.ds(0, T * LANES)], us.at[2 * LAYERS + 1])
    for gi in range(2 * LAYERS):
        bulk(full.at[gi, :, pl.ds(0, T * LANES)], cs.at[gi])
        if gi:
            bulk(full.at[gi, :, pl.ds(0, 3 * LANES)], us.at[gi + 1])
    for b in range(S):

        @pl.when(jnp.logical_not(final_here(b)))
        def _():
            fcopy(b, False).wait_send()

        for dt in range(T):

            @pl.when(jnp.logical_not(both(b == s, t == dt)))
            def _():
                qcopy(b, dt).wait_send()


def fused(mesh):
    S, T = mesh.shape["sp"], mesh.shape["tp"]

    def run(tokens, norm_gain, in_weight, gate_weight, conv_taps, decay_logit, gate_maps, out_weight, final_gain):
        rows, tcols = tokens.shape
        total = rows * S
        depth = D // 2
        dma = pltpu.SemaphoreType.DMA
        n = 2 * LAYERS
        vmem = pl.BlockSpec(memory_space=pltpu.VMEM)
        hbm = pl.BlockSpec(memory_space=pl.ANY)

        def body_of(*refs):
            kernel(S, T, *refs)

        return pl.pallas_call(
            body_of,
            out_shape=jax.ShapeDtypeStruct((rows, tcols), BF16),
            in_specs=[hbm] * 9,
            out_specs=vmem,
            scratch_shapes=[
                pltpu.VMEM((n, total, depth), BF16),
                pltpu.VMEM((rows, tcols), BF16),
                pltpu.VMEM((total, depth), BF16),
                pltpu.VMEM((LAYERS, 3, 2, 2, in_weight.shape[1] // 2, 2 * LANES), BF16),
                pltpu.VMEM((LAYERS, S, 2, LANES, LANES), BF16),
                pltpu.VMEM((LAYERS, depth), F32),
                pltpu.VMEM((1, tcols), F32),
                pltpu.VMEM((LAYERS, TAPS, tcols), F32),
                pltpu.VMEM((LAYERS, 2, tcols), F32),
                pltpu.VMEM((2, total, LANES), F32),
                pltpu.VMEM((LAYERS, 3, total, LANES), BF16),
                pltpu.VMEM((LAYERS, 3, total, LANES), BF16),
                pltpu.VMEM((LAYERS, 2, S, 8, LANES), F32),
                pltpu.VMEM((total, LANES), F32),
                pltpu.VMEM((total + 16, LANES), F32),
                pltpu.VMEM((LAYERS, 2, total, LANES), BF16),
                pltpu.VMEM((total, LANES), F32),
                pltpu.VMEM((total, LANES), BF16),
                pltpu.VMEM((S, 8, LANES), F32),
                pltpu.VMEM((S * T, 8, LANES), F32),
                pltpu.VMEM((rows, tcols), BF16),
                dma((LAYERS, 4)),
                dma((LAYERS, 4, 4)),
                dma((LAYERS, 4)),
                dma((LAYERS, 4)),
                dma((n + 2,)),
                dma((n, S, 3)),
                dma((n,)),
                dma((n, S)),
                dma((LAYERS, 3)),
                dma((LAYERS, 3, S)),
                dma((LAYERS,)),
                dma((LAYERS,)),
                dma((LAYERS,)),
                dma((LAYERS,)),
                dma((2, 2)),
                dma((2,)),
                dma((S,)),
                dma((1,)),
                dma((S, T)),
                dma((1,)),
                dma((3,)),
            ],
            compiler_params=pltpu.CompilerParams(
                collective_id=0, has_side_effects=True, vmem_limit_bytes=60 * 1024 * 1024
            ),
        )(tokens, norm_gain, in_weight, gate_weight, conv_taps, decay_logit, gate_maps, out_weight, final_gain.reshape(1, tcols))

    return run


def solution(mesh):
    placed = (
        P(("grp", "sp"), "tp"),
        P(),
        P(None, "sp", "tp"),
        P(None, "sp", "tp"),
        P(None, None, "tp"),
        P(None, None, "tp"),
        P(None, "tp", "sp"),
        P(None, "sp", "tp"),
        P("tp"),
    )
    shape = dict(mesh.shape)
    fits = (
        shape["grp"] == 2
        and shape["tp"] == 4
        and shape["sp"] == 4
        and D == shape["sp"] * shape["tp"] * LANES
        and HEAD_W == 2 * LANES
    )
    return jax.shard_map(
        fused(mesh) if fits else body, mesh=mesh, in_specs=placed, out_specs=P(("grp", "sp"), "tp"), check_vma=False
    )
```
